32 devices in a mesh: ep: 8 (over z, y), tp: 4 (over x, core).
Axes of the slice: x: 2, y: 2, z: 4, core: 2. Of those that a mesh axis runs over, the one named last changes fastest.
Arguments:
- queries_a: bfloat16 [1024, 1024], P('ep', 'tp'), may hold values from -128 to 128
- queries_b: bfloat16 [1024, 1024], P('ep', 'tp'), may hold values from -128 to 128
- keys_a: bfloat16 [1024, 512], P('ep', 'tp'), may hold values from -8 to 8
- keys_b: bfloat16 [1024, 512], P('ep', 'tp'), may hold values from -8 to 8
- values: bfloat16 [1024, 1024], P('ep', 'tp'), may hold values from -6 to 6
- lambdas: float32 [16], P('tp'), may hold values from 0.3 to 0.8
- head_gain: float32 [128], replicated, may hold values from 0.1 to 1.9
- w_out: bfloat16 [2048, 2048], P('tp'), may hold values from -0.125 to 0.125
- moe_tokens: bfloat16 [4096, 2048], P(('ep', 'tp')), may hold values from -80 to 80
- moe_gain: float32 [2048], replicated, may hold values from 0.1 to 1.9
- routes: int32 [4096, 2], P(('ep', 'tp')), may hold values from 0 to 7, all different within a row; in each aligned block of 128 rows (0 to 127, 128 to 255, ...) at most 48 rows name the same one
- route_weights: float32 [4096, 2], P(('ep', 'tp')), may hold values from 0.1 to 1
- w_gate: bfloat16 [8, 2048, 2048], P('ep', None, 'tp'), may hold values from -4 to 4
- w_up: bfloat16 [8, 2048, 2048], P('ep', None, 'tp'), may hold values from -4 to 4
- w_down: bfloat16 [8, 2048, 2048], P('ep', 'tp'), may hold values from -0.0625 to 0.0625
Outputs:
- mixer_out: bfloat16 [1024, 2048], P(('ep', 'tp'))
- moe_out: bfloat16 [4096, 2048], P(('ep', 'tp'))
The draws below stay inside these ranges and needn't reach their ends.
Inputs may be any that keep to these rules, and one draw needn't show every extreme that they name: `routes`: each row names 2 different experts. Within the rows of one device no expert is named by more than 48 rows, a bound that some block reaches of some device.
All inputs are finite; a program needn't handle non-finite values.
Results may differ from the reference program's by a relative error of at most 0.011.
Values may be sent and summed in bfloat16 or wider, within the bound.
A program may use at most 192 MiB of HBM per device.

```python
import math
import jax
import jax.numpy as jnp
import numpy as np
from jax import lax

D = 2048
HEADS = 16
KV_HEADS = 8
HEAD = 64
VDIM = 128
FF = 2048
TOP = 2
ATT_DEV = 128
TOKB = 128
EXPERTS = 8
CAP = 48
SEQ = 1024
MOE_TOK = 4096
N_EP = 8
N_TP = 4


def query_key_pair(key, which):
    streams = jax.random.split(jax.random.fold_in(key, 1000 + which), 2)
    queries = 1.3 * jnp.clip(jax.random.normal(streams[0], (SEQ, HEADS * HEAD), jnp.float32), -4.0, 4.0)
    keys = 1.3 * jnp.clip(jax.random.normal(streams[1], (SEQ, KV_HEADS * HEAD), jnp.float32), -4.0, 4.0)
    return (queries, keys)


def draw_queries_a(key, part):
    return query_key_pair(key, 0)[0].astype(jnp.bfloat16)


def draw_keys_a(key, part):
    return query_key_pair(key, 0)[1].astype(jnp.bfloat16)


def draw_queries_b(key, part):
    return query_key_pair(key, 1)[0].astype(jnp.bfloat16)


def draw_keys_b(key, part):
    return query_key_pair(key, 1)[1].astype(jnp.bfloat16)


def draw_moe_tokens(key, part):
    streams = jax.random.split(jax.random.fold_in(key, 2000), 3)
    base = jnp.clip(jax.random.normal(streams[0], (MOE_TOK, D), jnp.float32), -4.0, 4.0)
    row_scale = jnp.exp(jax.random.uniform(streams[1], (MOE_TOK, 1), jnp.float32, math.log(0.3), math.log(3.0)))
    column_scale = jnp.exp(jax.random.uniform(streams[2], (1, D), jnp.float32, math.log(0.3), math.log(3.0)))
    result = base * row_scale * column_scale
    return result.astype(jnp.bfloat16)


def expert_matrix(key, salt):
    streams = jax.random.split(jax.random.fold_in(key, salt), 2)
    base = jnp.clip(jax.random.normal(streams[0], (EXPERTS, D, FF), jnp.float32), -4.0, 4.0) / math.sqrt(D)
    spread = jax.random.uniform(streams[1], (EXPERTS, 1, FF), jnp.float32, math.log(0.3), math.log(4.0))
    return (base * jnp.exp(spread)).astype(jnp.bfloat16)


def draw_w_gate(key, part):
    return expert_matrix(key, 3000)


def draw_w_up(key, part):
    return expert_matrix(key, 4000)


def block_scale(stream_key, extent, cuts, least, high):
    gain, own = 1.0, jax.random.fold_in(stream_key, 6)
    for position, parts in cuts:
        heights = jnp.exp(jax.random.uniform(jax.random.fold_in(own, position), (parts,), jnp.float32, least / len(cuts), high / len(cuts)))
        gain = gain * jnp.repeat(heights, extent[position] // parts).reshape([-1 if axis == position else 1 for axis in range(len(extent))])
    return gain


def deal_out(stream_key, own, number, rows, number_of, top, limit, skew):
    sequence = jax.random.permutation(stream_key, number_of)
    heavy_load, ordinary = shares(number_of, rows * top, limit, skew, True), shares(number_of, rows * top, limit, skew, False)
    places = jnp.arange(number_of)

    def named(tallies, offset_by):
        used = int((tallies > 0).sum())
        fixed = max(1, used // 4)
        shifted = fixed + (places - fixed + offset_by * (used - fixed)) % max(1, number_of - fixed)
        return jnp.zeros((number_of,), jnp.int32).at[sequence[jnp.where(places < fixed, places, shifted)]].set(jnp.asarray(tallies, jnp.int32))

    tallies = jnp.where(number % 4 == 0, named(heavy_load, number // 4), named(ordinary, number - number // 4 - 1))
    mixed = jax.random.permutation(jax.random.fold_in(own, 3), number_of)
    source_of, taker = mixed[0:number_of // 2 * 2:2], mixed[1:number_of // 2 * 2:2]
    slack = jnp.minimum(tallies[source_of] - 1, limit - tallies[taker]) // 2
    slack = jnp.where((source_of == sequence[0]) | (taker == sequence[0]) | (tallies[taker] == 0), 0, jnp.maximum(slack, 0))
    shifted = jax.random.randint(jax.random.fold_in(own, 4), (number_of // 2,), 0, 1 << 20) % (slack + 1)
    tallies = tallies.at[source_of].add(-shifted).at[taker].add(shifted)
    items = jnp.searchsorted(jnp.cumsum(tallies), jnp.arange(rows * top), side="right").astype(jnp.int32)
    grid = items.reshape(top, rows).T
    grid = grid[jax.random.permutation(jax.random.fold_in(own, 1), rows)]
    offset_by = jax.random.randint(jax.random.fold_in(own, 2), (rows, 1), 0, top)
    return jnp.take_along_axis(grid, (jnp.arange(top)[None, :] + offset_by) % top, axis=1)


def shares(number_of, total, most, slope, full):
    weights = [(1 << 20) // math.isqrt(rank ** slope) + 1 for rank in range(1, number_of + 1)]
    largest = most if full else min(most, max(-(-total // number_of), total * weights[0] // sum(weights)))
    least = 1 if total - largest >= number_of - 1 else 0
    given, rest = [largest] + [least] * (number_of - 1), total - largest - least * (number_of - 1)
    while rest > 0:
        free = [i for i in range(1, number_of) if given[i] < largest] or [i for i in range(1, number_of) if given[i] < most]
        whole, remaining = sum([weights[i] for i in free]), rest
        for i in free:
            addition = min(most - given[i], max(1, remaining * weights[i] // whole), rest)
            given[i] = given[i] + addition
            rest = rest - addition
    return np.array(given)


def bell_draw(key, shape, deviation, limit, shards=(), held_as=jnp.bfloat16):
    drawn = deviation * jax.random.normal(key, shape, jnp.float32)
    if shards:
        drawn = drawn * block_scale(key, shape, shards, -0.22, 0.18)
    return jnp.clip(drawn, -limit, limit).astype(held_as)


def setup_inputs(seed: int = 0) -> dict:
    key_list = jax.random.split(jax.random.key(seed), 16)
    queries_a = draw_queries_a(jax.random.fold_in(key_list[15], 71), 0)
    queries_b = draw_queries_b(jax.random.fold_in(key_list[15], 71), 0)
    keys_a = draw_keys_a(jax.random.fold_in(key_list[15], 71), 0)
    keys_b = draw_keys_b(jax.random.fold_in(key_list[15], 71), 0)
    values = bell_draw(key_list[4], (SEQ, KV_HEADS * VDIM), 1.0, 6.0, ((0, 8), (1, 4)))
    lambdas = jnp.clip(0.3 + 0.5 * jax.random.uniform(key_list[5], (HEADS,), jnp.float32) ** block_scale(key_list[5], (HEADS,), ((0, 4),), -0.2, 0.2), 0.3, 0.8)
    head_gain = jnp.clip(1.0 + 0.18 * jax.random.normal(key_list[6], (VDIM,), jnp.float32), 0.1, 1.9)
    w_out = bell_draw(key_list[7], (HEADS * VDIM, D), (HEADS * VDIM) ** -0.5, 0.125, ((0, 4),))
    moe_tokens = draw_moe_tokens(jax.random.fold_in(key_list[15], 71), 0)
    moe_gain = jnp.clip(1.0 + 0.18 * jax.random.normal(key_list[9], (D,), jnp.float32), 0.1, 1.9)
    routes_keys = jax.random.split(jax.random.fold_in(key_list[10], 1), MOE_TOK // TOKB)
    routes_turns = jax.random.permutation(jax.random.fold_in(key_list[10], 3), MOE_TOK // TOKB)
    routes = jax.vmap(lambda own, number: deal_out(jax.random.fold_in(key_list[10], 2), own, number, TOKB, EXPERTS, TOP, CAP, 2))(routes_keys, routes_turns).reshape((MOE_TOK, TOP))
    route_weights = jnp.clip(0.1 + 0.9 * jax.random.uniform(key_list[11], (MOE_TOK, TOP), jnp.float32) ** block_scale(key_list[11], (MOE_TOK, TOP), ((0, 32),), -0.2, 0.2), 0.1, 1.0)
    w_gate = draw_w_gate(jax.random.fold_in(key_list[15], 71), 0)
    w_up = draw_w_up(jax.random.fold_in(key_list[15], 71), 0)
    w_down = bell_draw(key_list[14], (EXPERTS, FF, D), (4 * FF) ** -0.5, 0.0625, ((0, 8), (1, 4)))
    return {"queries_a": queries_a, "queries_b": queries_b, "keys_a": keys_a, "keys_b": keys_b, "values": values, "lambdas": lambdas, "head_gain": head_gain, "w_out": w_out, "moe_tokens": moe_tokens, "moe_gain": moe_gain, "routes": routes, "route_weights": route_weights, "w_gate": w_gate, "w_up": w_up, "w_down": w_down}


eps = 1e-05
alpha_act = 1.702
limit_act = 7.0

def clamped_unit(gate, up):
    capped = jnp.minimum(gate, limit_act)
    linear = jnp.clip(up, -limit_act, limit_act)
    return capped * jax.nn.sigmoid(alpha_act * capped) * (linear + 1.0)

def hidden_rows(inputs, gate_matrix, up_matrix):
    gate = jnp.dot(inputs, gate_matrix, preferred_element_type=jnp.float32)
    up = jnp.dot(inputs, up_matrix, preferred_element_type=jnp.float32)
    return clamped_unit(gate, up).astype(jnp.bfloat16)

def map_weights(queries, keys, value_rows, query_pos, key_pos):
    scores = jnp.dot(queries, keys.T, preferred_element_type=jnp.float32) * HEAD ** (-0.5)
    visible = key_pos[None, :] <= query_pos[:, None]
    scores = jnp.where(visible, scores, -jnp.inf)
    peak = lax.optimization_barrier(jnp.max(scores, axis=1, keepdims=True))
    expo = jnp.where(visible, jnp.exp(scores - peak), 0.0)
    total = lax.optimization_barrier(jnp.sum(expo, axis=1, keepdims=True))
    mixed = jnp.dot(expo.astype(jnp.bfloat16), value_rows, preferred_element_type=jnp.float32)
    return mixed / total

def one_head(head, queries_a, queries_b, keys_a, keys_b, values, lambdas, head_gain):
    kv_head = head // (HEADS // KV_HEADS)
    query_a = lax.dynamic_slice_in_dim(queries_a, (head * HEAD).astype(jnp.int32), HEAD, 1)
    query_b = lax.dynamic_slice_in_dim(queries_b, (head * HEAD).astype(jnp.int32), HEAD, 1)
    key_a = lax.dynamic_slice_in_dim(keys_a, (kv_head * HEAD).astype(jnp.int32), HEAD, 1)
    key_b = lax.dynamic_slice_in_dim(keys_b, (kv_head * HEAD).astype(jnp.int32), HEAD, 1)
    value_head = lax.dynamic_slice_in_dim(values, (kv_head * VDIM).astype(jnp.int32), VDIM, 1)
    key_pos = jnp.arange(SEQ, dtype=jnp.int32)
    strength = lambdas[head]

    def one_block(index):
        start = (index * ATT_DEV).astype(jnp.int32)
        query_pos = start + jnp.arange(ATT_DEV, dtype=jnp.int32)
        first = map_weights(lax.dynamic_slice_in_dim(query_a, start, ATT_DEV, 0), key_a, value_head, query_pos, key_pos)
        second = map_weights(lax.dynamic_slice_in_dim(query_b, start, ATT_DEV, 0), key_b, value_head, query_pos, key_pos)
        diff = first - strength * second
        scaled = diff * lax.rsqrt(lax.optimization_barrier(jnp.mean(diff * diff, axis=-1, keepdims=True)) + eps) * head_gain
        return scaled.astype(jnp.bfloat16)
    return lax.map(one_block, jnp.arange(N_EP, dtype=jnp.int32)).reshape(SEQ, VDIM)

def reference(queries_a, queries_b, keys_a, keys_b, values, lambdas, head_gain, w_out, moe_tokens, moe_gain, routes, route_weights, w_gate, w_up, w_down):
    heads = lax.map(lambda head: one_head(head, queries_a, queries_b, keys_a, keys_b, values, lambdas, head_gain), jnp.arange(HEADS, dtype=jnp.int32))
    heads = heads.transpose(1, 0, 2).reshape(SEQ, N_TP, HEADS // N_TP * VDIM)
    weight_groups = w_out.reshape(N_TP, HEADS // N_TP * VDIM, D)
    head_parts = jnp.einsum('sjc,jcd->jsd', heads.astype(jnp.float32), weight_groups.astype(jnp.float32))
    head_parts = lax.optimization_barrier(head_parts.astype(jnp.bfloat16))
    mixer_out = lax.optimization_barrier(jnp.sum(head_parts.astype(jnp.float32), axis=0)).astype(jnp.bfloat16)
    inputs = moe_tokens.astype(jnp.float32)
    normed = (inputs * lax.rsqrt(lax.optimization_barrier(jnp.mean(inputs * inputs, axis=-1, keepdims=True)) + eps) * moe_gain).astype(jnp.bfloat16)
    blocks = MOE_TOK // TOKB
    chosen = routes.reshape(blocks, TOKB * TOP)
    member = (chosen[:, :, None] == jnp.arange(EXPERTS, dtype=jnp.int32)[None, None, :]).astype(jnp.int32)
    order_in = lax.optimization_barrier(jnp.sum(jnp.cumsum(member, axis=1) * member, axis=2)) - 1
    block_ids = jnp.arange(blocks, dtype=jnp.int32)[:, None]
    slot_ids = ((chosen * blocks + block_ids) * CAP + order_in).astype(jnp.int32)
    token_ids = (block_ids * TOKB + jnp.arange(TOKB * TOP, dtype=jnp.int32)[None, :] // TOP).astype(jnp.int32)
    owner = jnp.full((EXPERTS * blocks * CAP,), MOE_TOK, jnp.int32).at[slot_ids.reshape(-1)].set(token_ids.reshape(-1))
    owner = owner.reshape(EXPERTS, blocks * CAP)

    def one_expert(index):
        slot_owner = owner[index]
        valid = slot_owner < MOE_TOK
        taken = jnp.take(normed, jnp.minimum(slot_owner, MOE_TOK - 1), axis=0)
        taken = jnp.where(valid[:, None], taken, jnp.zeros_like(taken))
        hidden = hidden_rows(taken, w_gate[index], w_up[index])
        unit_parts = jnp.einsum('rjf,jfd->jrd', hidden.reshape(-1, N_TP, FF // N_TP).astype(jnp.float32), w_down[index].reshape(N_TP, FF // N_TP, D).astype(jnp.float32))
        unit_parts = lax.optimization_barrier(unit_parts.astype(jnp.bfloat16))
        return lax.optimization_barrier(jnp.sum(unit_parts.astype(jnp.float32), axis=0)).astype(jnp.bfloat16)
    expert_rows = lax.map(one_expert, jnp.arange(EXPERTS, dtype=jnp.int32))
    picked = jnp.take(expert_rows.reshape(-1, D), slot_ids.reshape(-1), axis=0).reshape(MOE_TOK, TOP, D)
    moe_out = lax.optimization_barrier(jnp.sum(picked.astype(jnp.float32) * route_weights[:, :, None], axis=1)).astype(jnp.bfloat16)
    return (mixer_out, moe_out)
```

```python
import functools

import jax
import jax.numpy as jnp
from jax import lax
from jax.experimental import pallas as pl
from jax.experimental.pallas import tpu as pltpu
from jax.sharding import PartitionSpec as P

HEAD = 64
VDIM = 128
TOP = 2


eps = 1e-05
alpha_act = 1.702
limit_act = 7.0
negative = -1e30


def clamped_unit(gate, up):
    capped = jnp.minimum(gate, limit_act)
    linear = jnp.clip(up, -limit_act, limit_act)
    return capped * jax.nn.sigmoid(alpha_act * capped) * (linear + 1.0)


def hidden_rows(inputs, gate_matrix, up_matrix):
    gate = jnp.dot(inputs, gate_matrix, preferred_element_type=jnp.float32)
    up = jnp.dot(inputs, up_matrix, preferred_element_type=jnp.float32)
    return clamped_unit(gate, up).astype(jnp.bfloat16)


def pick_rows(table, owner):
    valid = owner < table.shape[0]
    chosen = jnp.take(table, jnp.minimum(owner, table.shape[0] - 1), axis=0)
    return jnp.where(valid[:, None], chosen, jnp.zeros_like(chosen))


def mixer(queries_a, queries_b, keys_a, keys_b, values, lambdas, head_gain, w_out):
    tokens = queries_a.shape[0]
    local_heads = lambdas.shape[0]
    kv_local = keys_a.shape[1] // HEAD
    group = local_heads // kv_local
    scale = HEAD ** (-0.5)
    query_pos = lax.axis_index("ep") * tokens + jnp.arange(tokens, dtype=jnp.int32)
    grouped_a = queries_a.reshape(tokens, kv_local, group, HEAD)
    grouped_b = queries_b.reshape(tokens, kv_local, group, HEAD)
    lowest = jnp.full((kv_local, group, tokens), negative, jnp.float32)
    nothing = jnp.zeros((kv_local, group, tokens), jnp.float32)
    blank = jnp.zeros((kv_local, group, tokens, VDIM), jnp.float32)

    def one_map(grouped, keys, value_rows, visible, state):
        peak, total, accum = state
        scores = (
            jnp.einsum("rgjd,ngd->gjrn", grouped, keys, preferred_element_type=jnp.float32) * scale
        )
        scores = jnp.where(visible, scores, negative)
        new_peak = jnp.maximum(peak, jnp.max(scores, axis=-1))
        expo = jnp.where(visible, jnp.exp(scores - new_peak[..., None]), 0.0)
        total = jnp.sum(expo, axis=-1)
        accum = jnp.einsum(
            "gjrn,ngv->gjrv",
            expo.astype(jnp.bfloat16),
            value_rows,
            preferred_element_type=jnp.float32,
        )
        return (new_peak, total, accum)

    initial = (lowest, nothing, blank, lowest, nothing, blank)
    piece_a = lax.all_gather(keys_a, "ep", axis=0, tiled=True)
    piece_b = lax.all_gather(keys_b, "ep", axis=0, tiled=True)
    piece_v = lax.all_gather(values, "ep", axis=0, tiled=True)
    count = piece_a.shape[0]

    def visit(state):
        key_pos = jnp.arange(count, dtype=jnp.int32)
        visible = key_pos[None, :] <= query_pos[:, None]
        value_rows = piece_v.reshape(count, kv_local, VDIM)
        first = one_map(
            grouped_a, piece_a.reshape(count, kv_local, HEAD), value_rows, visible, state[:3]
        )
        second = one_map(
            grouped_b, piece_b.reshape(count, kv_local, HEAD), value_rows, visible, state[3:]
        )
        return first + second

    result = lax.cond(jnp.int32(0) <= query_pos[tokens - 1], visit, lambda state: state, initial)
    mixed_a = result[2] / result[1][..., None]
    mixed_b = result[5] / result[4][..., None]
    diff = mixed_a - lambdas.reshape(kv_local, group, 1, 1) * mixed_b
    heads_out = (
        diff * lax.rsqrt(jnp.mean(diff * diff, axis=-1, keepdims=True) + eps) * head_gain
    ).astype(jnp.bfloat16)
    weights_out = w_out.reshape(kv_local, group, VDIM, w_out.shape[1])
    return lax.psum_scatter(
        jnp.einsum(
            "gjrv,gjvd->rd", heads_out, weights_out, preferred_element_type=jnp.float32
        ).astype(jnp.bfloat16),
        "tp",
        scatter_dimension=0,
        tiled=True,
    )


def experts(moe_tokens, moe_gain, routes, route_weights, w_gate, w_up, w_down):
    tok_rows, width = moe_tokens.shape
    n_experts = lax.axis_size("ep") * w_gate.shape[0]
    capacity = max(2, 3 * tok_rows * TOP // (2 * n_experts))
    inputs = moe_tokens.astype(jnp.float32)
    normed = (
        inputs * lax.rsqrt(jnp.mean(inputs * inputs, axis=-1, keepdims=True) + eps) * moe_gain
    ).astype(jnp.bfloat16)
    chosen = routes.reshape(-1)
    member = (chosen[:, None] == jnp.arange(n_experts, dtype=jnp.int32)[None, :]).astype(jnp.int32)
    order_in = jnp.sum(jnp.cumsum(member, axis=0) * member, axis=1) - 1
    slot_ids = chosen * capacity + order_in
    owner = (
        jnp.full((n_experts * capacity,), tok_rows, jnp.int32)
        .at[slot_ids]
        .set(jnp.arange(tok_rows * TOP, dtype=jnp.int32) // TOP)
    )
    outgoing = pick_rows(normed, owner).reshape(n_experts, capacity, width)
    arrived = lax.all_to_all(outgoing, "ep", split_axis=0, concat_axis=1, tiled=True).reshape(
        -1, width
    )
    hidden = hidden_rows(lax.all_gather(arrived, "tp", axis=0, tiled=True), w_gate[0], w_up[0])
    expert_out = lax.psum_scatter(
        jnp.dot(hidden, w_down[0], preferred_element_type=jnp.float32).astype(jnp.bfloat16),
        "tp",
        scatter_dimension=0,
        tiled=True,
    )
    returned = lax.all_to_all(
        expert_out.reshape(-1, capacity, width), "ep", split_axis=0, concat_axis=0, tiled=True
    )
    picked = jnp.take(returned.reshape(-1, width), slot_ids, axis=0).reshape(tok_rows, TOP, width)
    return jnp.sum(picked.astype(jnp.float32) * route_weights[:, :, None], axis=1).astype(
        jnp.bfloat16
    )


def body(
    queries_a,
    queries_b,
    keys_a,
    keys_b,
    values,
    lambdas,
    head_gain,
    w_out,
    moe_tokens,
    moe_gain,
    routes,
    route_weights,
    w_gate,
    w_up,
    w_down,
):
    mixer_out = mixer(queries_a, queries_b, keys_a, keys_b, values, lambdas, head_gain, w_out)
    moe_out = experts(moe_tokens, moe_gain, routes, route_weights, w_gate, w_up, w_down)
    return (mixer_out, moe_out)


MESH = pl.DeviceIdType.MESH
OUT, CORE, ACROSS, CORE_ACROSS, PART, PAIR, SUMS, BACK, KV_Z, KV_Y, MIX = range(11)


def xor(first, second, limit):
    total, bit = 0, 1
    while bit < limit:
        total = total + (first // bit + second // bit) % 2 * bit
        bit *= 2
    return total


def exchange(
    n, tokens_in, moe_gain, routes, route_weights, queries_a, queries_b, head_gain, lambdas,
    keys_a, keys_b, values, w_gate, w_up, w_down, w_out,
    moe_out, mixer_out,
    ret, outgoing, weigh, rows, parts, part_in, pair_in, sums_in, sums, final, hidden, gate_v, up_v, down_v, out_v,
    kv_all, heads, shares, mix_part, mix_pair, mix_in, mix_sum, send, recv, local,
):
    me = lax.axis_index("ep")
    tp = lax.axis_index("tp")
    core = tp + 1 - 2 * (tp % 2)
    across = tp + 2 - 4 * (tp // 2)
    diagonal = core + 2 - 4 * (core // 2)
    floor, lane = me // 2, me % 2
    floors = n // 2
    cap, width = outgoing.shape[1:]
    units = hidden.shape[1]
    flat = 4 * cap
    tokens = kv_all.shape[1]

    def mask_of(k):
        return 2 * ((n // 2 - k // 2) % (n // 2)) + k % 2

    def partner(k):
        return xor(me, mask_of(k), n)

    def copy(kind, k, source, target, device):
        return pltpu.make_async_remote_copy(
            src_ref=source,
            dst_ref=target,
            send_sem=send.at[kind, k],
            recv_sem=recv.at[kind, k],
            device_id=device,
            device_id_type=MESH,
        )

    def out_copy(k):
        return copy(OUT, k, outgoing.at[partner(k)], rows.at[k, 0], {"ep": partner(k)})

    def core_copy(k):
        return copy(CORE, k, rows.at[k, 0], rows.at[k, 1], {"tp": core})

    def across_copy(k):
        return copy(ACROSS, k, rows.at[k, 0], rows.at[k, 2], {"tp": across})

    def core_across_copy(k):
        return copy(CORE_ACROSS, k, rows.at[k, 2], rows.at[k, 3], {"tp": core})

    def part_copy(k):
        return copy(PART, k, parts.at[k, 1], part_in.at[k], {"tp": core})

    def pair_copy(k):
        return copy(PAIR, k, parts.at[k, 3], pair_in.at[k], {"tp": core})

    def sums_copy(k):
        return copy(SUMS, k, sums.at[k], sums_in.at[k], {"tp": across})

    def back_copy(k):
        return copy(BACK, k, final.at[k], ret.at[me], {"ep": partner(k)})

    def kv_z_copy(stage):
        block = kv_all.at[2 * (floor - stage + 1) + lane]
        return copy(KV_Z, stage, block, block, {"ep": me + 2})

    def kv_y_copy(stage):
        block = kv_all.at[2 * (floor - stage) + lane]
        return copy(KV_Y, stage, block, block, {"ep": me + 1 - 2 * lane})

    mix_part_copy = copy(MIX, 0, shares.at[core], mix_part, {"tp": core})
    mix_pair_copy = copy(MIX, 1, shares.at[diagonal], mix_pair, {"tp": core})
    mix_sum_copy = copy(MIX, 2, mix_sum, mix_in, {"tp": across})

    local_heads = heads.shape[1] // VDIM
    kv_local = kv_all.shape[2] // (2 * HEAD + VDIM)
    span = kv_local * HEAD

    def one_map(queries, head, offset):
        g = head // (local_heads // kv_local)
        count = n * tokens
        first = offset + g * HEAD
        keys = kv_all[:, :, first : first + HEAD].reshape(count, HEAD)
        first = 2 * span + g * VDIM
        value_rows = kv_all[:, :, first : first + VDIM].reshape(count, VDIM)
        scores = lax.dot_general(
            queries[:, head * HEAD : (head + 1) * HEAD],
            keys,
            (((1,), (1,)), ((), ())),
            preferred_element_type=jnp.float32,
        ) * HEAD ** (-0.5)
        query_pos = me * tokens + lax.broadcasted_iota(jnp.int32, scores.shape, 0)
        key_pos = lax.broadcasted_iota(jnp.int32, scores.shape, 1)
        scores = jnp.where(key_pos <= query_pos, scores, negative)
        expo = jnp.exp(scores - jnp.max(scores, axis=1, keepdims=True))
        total = jnp.sum(expo, axis=1, keepdims=True)
        mixed = jnp.dot(
            expo.astype(jnp.bfloat16), value_rows, preferred_element_type=jnp.float32
        )
        return mixed / total

    def attend(head):
        diff = one_map(queries_a, head, 0) - lambdas[head] * one_map(queries_b, head, span)
        norm = lax.rsqrt(jnp.mean(diff * diff, axis=1, keepdims=True) + eps)
        heads[:, head * VDIM : (head + 1) * VDIM] = (diff * norm * head_gain[...]).astype(
            jnp.bfloat16
        )

    def forward(k):
        core_copy(k).start()
        across_copy(k).start()

    def relay(k):
        across_copy(k).wait_recv()
        core_across_copy(k).start()

    def send_sums(k):
        pair_copy(k).wait_recv()
        sums[k] = (
            parts[k, 2].astype(jnp.float32) + pair_in[k].astype(jnp.float32)
        ).astype(jnp.bfloat16)
        sums_copy(k).start()

    def finish(k):
        part_copy(k).wait_recv()
        sums_copy(k).wait_recv()
        return (
            parts[k, 0].astype(jnp.float32)
            + part_in[k].astype(jnp.float32)
            + sums_in[k].astype(jnp.float32)
        ).astype(jnp.bfloat16)

    def send_back(k):
        final[k] = finish(k)
        back_copy(k).start()

    def feed(k):
        core_copy(k).wait_recv()
        core_across_copy(k).wait_recv()
        inputs = rows[k].reshape(flat, width)
        step = min(256, units)
        for first in range(0, units, step):
            gate = jnp.dot(
                inputs, gate_v[:, first : first + step], preferred_element_type=jnp.float32
            )
            up = jnp.dot(
                inputs, up_v[:, first : first + step], preferred_element_type=jnp.float32
            )
            hidden[:, first : first + step] = clamped_unit(gate, up).astype(jnp.bfloat16)
        for first in range(0, width, 256):
            piece = jnp.dot(
                hidden[...], down_v[:, first : first + 256], preferred_element_type=jnp.float32
            )
            parts[k, :, :, first : first + 256] = piece.astype(jnp.bfloat16).reshape(
                4, cap, 256
            )
        pair_copy(k).start()
        part_copy(k).start()

    barrier = pltpu.get_barrier_semaphore()
    for shift in range(1, n):
        pl.semaphore_signal(
            barrier, inc=1, device_id={"ep": (me + shift) % n}, device_id_type=MESH
        )
    for shift in range(1, 4):
        pl.semaphore_signal(
            barrier, inc=1, device_id={"tp": (tp + shift) % 4}, device_id_type=MESH
        )

    loads = [
        pltpu.make_async_copy(keys_a, kv_all.at[me, :, 0:span], local.at[0]),
        pltpu.make_async_copy(keys_b, kv_all.at[me, :, span : 2 * span], local.at[1]),
        pltpu.make_async_copy(values, kv_all.at[me, :, 2 * span :], local.at[2]),
        pltpu.make_async_copy(w_gate, gate_v, local.at[3]),
        pltpu.make_async_copy(w_up, up_v, local.at[4]),
        pltpu.make_async_copy(w_down, down_v, local.at[5]),
        pltpu.make_async_copy(w_out, out_v, local.at[6]),
    ]
    for load in loads:
        load.start()

    inputs = tokens_in[...].astype(jnp.float32)
    normed = (
        inputs
        * lax.rsqrt(jnp.mean(inputs * inputs, axis=1, keepdims=True) + eps)
        * moe_gain[...]
    ).astype(jnp.bfloat16)
    count = tokens_in.shape[0]
    expert = lax.broadcasted_iota(jnp.int32, (n, count), 0)
    named = [routes[k : k + 1, :] == expert for k in range(TOP)]
    member = named[0]
    for k in range(1, TOP):
        member = member | named[k]
    earlier = lax.broadcasted_iota(jnp.int32, (count, count), 0) < lax.broadcasted_iota(
        jnp.int32, (count, count), 1
    )
    place = jnp.dot(
        jnp.where(member, 1.0, 0.0).astype(jnp.bfloat16),
        jnp.where(earlier, 1.0, 0.0).astype(jnp.bfloat16),
        preferred_element_type=jnp.float32,
    )
    position = lax.broadcasted_iota(jnp.int32, (cap, count), 0).astype(jnp.float32)
    slot = jnp.where(member, place, -1.0)
    for e in range(n):
        pick = jnp.where(slot[e : e + 1, :] == position, 1.0, 0.0).astype(jnp.bfloat16)
        outgoing[e] = jnp.dot(pick, normed, preferred_element_type=jnp.float32).astype(
            jnp.bfloat16
        )
    rows[0, 0] = outgoing[me]
    pl.semaphore_wait(barrier, n + 2)

    forward(0)

    @pl.loop(1, n - 2)
    def _(k):
        out_copy(k).start()

    for load in loads[:3]:
        load.wait()

    @pl.when(floor < floors - 1)
    def _():
        kv_z_copy(1).start()

    for k in range(n - 2, n):
        out_copy(k).start()
    kv_y_copy(0).start()

    for other in range(1, floors):

        @pl.when(floor < other)
        def _():
            for side in range(2):
                kv_all[2 * other + side] = jnp.zeros(kv_all.shape[1:], jnp.bfloat16)

    share = route_weights[...]
    scale = jnp.where(named[0], share[0:1, :], 0.0)
    for k in range(1, TOP):
        scale = scale + jnp.where(named[k], share[k : k + 1, :], 0.0)
    for e in range(n):
        weight = jnp.where(slot[e : e + 1, :] == position, scale[e : e + 1, :], 0.0)
        high = weight.astype(jnp.bfloat16)
        weigh[0, e] = high
        weigh[1, e] = (weight - high.astype(jnp.float32)).astype(jnp.bfloat16)
    for load in loads[3:]:
        load.wait()

    def kv_next(stage):
        @pl.when(floor >= stage)
        def _():
            kv_z_copy(stage).wait_recv()
            kv_y_copy(stage).start()
            if stage < floors - 1:

                @pl.when(floor < floors - 1)
                def _():
                    kv_z_copy(stage + 1).start()

    @pl.loop(0, n)
    def _(k):
        @pl.when(k >= 2)
        def _():
            send_sums(k - 1)

        @pl.when(k >= 3)
        def _():
            send_back(k - 2)

        @pl.when(k + 1 < n)
        def _():
            out_copy(k + 1).wait_recv()
            forward(k + 1)

        relay(k)
        feed(k)

        for stage in range(1, floors):

            @pl.when(k == n - floors + stage)
            def _():
                kv_next(stage)

    send_sums(n - 1)
    send_sums(0)
    send_back(n - 2)
    for stage in range(floors):

        @pl.when(floor >= stage)
        def _():
            kv_y_copy(stage).wait_recv()

    for head in range(local_heads):
        attend(head)
    send_back(n - 1)
    for first in range(0, width, 256):
        piece = jnp.dot(
            heads[...], out_v[:, first : first + 256], preferred_element_type=jnp.float32
        )
        shares[:, :, first : first + 256] = piece.astype(jnp.bfloat16).reshape(
            4, tokens // 4, 256
        )
    mix_pair_copy.start()
    mix_part_copy.start()
    mix_pair_copy.wait_recv()
    mix_sum[...] = (
        shares[across].astype(jnp.float32) + mix_pair[...].astype(jnp.float32)
    ).astype(jnp.bfloat16)
    mix_sum_copy.start()
    ret[me] = finish(0)

    @pl.loop(1, n)
    def _(k):
        back_copy(k).wait_recv()

    picks = [weigh[k].reshape(n * cap, count) for k in range(2)]
    for first in range(0, width, 256):
        table = ret[:, :, first : first + 256].reshape(n * cap, 256)
        total = 0.0
        for k in range(2):
            total = total + lax.dot_general(
                picks[k], table, (((0,), (0,)), ((), ())), preferred_element_type=jnp.float32
            )
        moe_out[:, first : first + 256] = total.astype(jnp.bfloat16)

    mix_part_copy.wait_recv()
    mix_sum_copy.wait_recv()
    mixer_out[...] = (
        shares[tp].astype(jnp.float32)
        + mix_part[...].astype(jnp.float32)
        + mix_in[...].astype(jnp.float32)
    ).astype(jnp.bfloat16)

    for made in (mix_part_copy, mix_pair_copy, mix_sum_copy):
        made.wait_send()
    for stage in range(1, floors):

        @pl.when((floor >= stage - 1) & (floor < floors - 1))
        def _():
            kv_z_copy(stage).wait_send()

    for stage in range(floors):

        @pl.when(floor >= stage)
        def _():
            kv_y_copy(stage).wait_send()

    @pl.loop(0, n)
    def _(k):
        for made in (core_copy, across_copy, core_across_copy, part_copy, pair_copy, sums_copy):
            made(k).wait_send()

        @pl.when(k >= 1)
        def _():
            out_copy(k).wait_send()
            back_copy(k).wait_send()


def run_exchange(
    n, cap, tokens_in, moe_gain, routes, route_weights, queries_a, queries_b, head_gain,
    lambdas, keys_a, keys_b, values, w_gate, w_up, w_down, w_out,
):
    count, width = tokens_in.shape
    units = w_gate.shape[1]
    block = (n, cap, width)
    tokens = keys_a.shape[0]
    kv_width = keys_a.shape[1] + keys_b.shape[1] + values.shape[1]
    quarter = (tokens // 4, width)
    vmem = pl.BlockSpec(memory_space=pltpu.VMEM)
    hbm = pl.BlockSpec(memory_space=pl.ANY)
    return pl.pallas_call(
        functools.partial(exchange, n),
        out_shape=(
            jax.ShapeDtypeStruct((count, width), jnp.bfloat16),
            jax.ShapeDtypeStruct(quarter, jnp.bfloat16),
        ),
        in_specs=[vmem] * 7 + [pl.BlockSpec(memory_space=pltpu.SMEM)] + [hbm] * 7,
        out_specs=(vmem, vmem),
        scratch_shapes=[
            pltpu.VMEM(block, jnp.bfloat16),
            pltpu.VMEM(block, jnp.bfloat16),
            pltpu.VMEM((2, n, cap, count), jnp.bfloat16),
            pltpu.VMEM((n, 4, cap, width), jnp.bfloat16),
            pltpu.VMEM((n, 4, cap, width), jnp.bfloat16),
            pltpu.VMEM(block, jnp.bfloat16),
            pltpu.VMEM(block, jnp.bfloat16),
            pltpu.VMEM(block, jnp.bfloat16),
            pltpu.VMEM(block, jnp.bfloat16),
            pltpu.VMEM(block, jnp.bfloat16),
            pltpu.VMEM((4 * cap, units), jnp.bfloat16),
            pltpu.VMEM(w_gate.shape, jnp.bfloat16),
            pltpu.VMEM(w_up.shape, jnp.bfloat16),
            pltpu.VMEM(w_down.shape, jnp.bfloat16),
            pltpu.VMEM(w_out.shape, jnp.bfloat16),
            pltpu.VMEM((n, tokens, kv_width), jnp.bfloat16),
            pltpu.VMEM((tokens, w_out.shape[0]), jnp.bfloat16),
            pltpu.VMEM((4,) + quarter, jnp.bfloat16),
            pltpu.VMEM(quarter, jnp.bfloat16),
            pltpu.VMEM(quarter, jnp.bfloat16),
            pltpu.VMEM(quarter, jnp.bfloat16),
            pltpu.VMEM(quarter, jnp.bfloat16),
            pltpu.SemaphoreType.DMA((11, n)),
            pltpu.SemaphoreType.DMA((11, n)),
            pltpu.SemaphoreType.DMA((7,)),
        ],
        compiler_params=pltpu.CompilerParams(
            collective_id=0, has_side_effects=True, vmem_limit_bytes=60 * 2**20
        ),
        name="exchange",
    )(
        tokens_in, moe_gain.reshape(1, -1), routes.T, route_weights.T,
        queries_a, queries_b, head_gain.reshape(1, -1), lambdas,
        keys_a, keys_b, values, w_gate, w_up, w_down, w_out,
    )


def fast_body(
    queries_a, queries_b, keys_a, keys_b, values, lambdas, head_gain, w_out,
    moe_tokens, moe_gain, routes, route_weights, w_gate, w_up, w_down,
):
    n = lax.axis_size("ep")
    cap = 3 * moe_tokens.shape[0] * TOP // (2 * n)
    moe_out, mixer_out = run_exchange(
        n, cap, moe_tokens, moe_gain, routes, route_weights, queries_a, queries_b,
        head_gain, lambdas, keys_a, keys_b, values, w_gate[0], w_up[0], w_down[0], w_out,
    )
    return (mixer_out, moe_out)


def whole_body(*args):
    n, n_tp = lax.axis_size("ep"), lax.axis_size("tp")
    tok_rows, w_gate = args[8].shape[0], args[12]
    cap = 3 * tok_rows * TOP // (2 * n)
    if w_gate.shape[0] == 1 and n_tp == 4 and n & (n - 1) == 0 and n >= 8 and cap % 16 == 0:
        return fast_body(*args)
    return body(*args)


def solution(mesh):
    return jax.shard_map(
        whole_body,
        mesh=mesh,
        in_specs=(
            P("ep", "tp"),
            P("ep", "tp"),
            P("ep", "tp"),
            P("ep", "tp"),
            P("ep", "tp"),
            P("tp"),
            P(),
            P("tp", None),
            P(("ep", "tp"), None),
            P(),
            P(("ep", "tp"), None),
            P(("ep", "tp"), None),
            P("ep", None, "tp"),
            P("ep", None, "tp"),
            P("ep", "tp", None),
        ),
        out_specs=(P(("ep", "tp"), None), P(("ep", "tp"), None)),
        check_vma=False,
    )
```

```python
import functools

import jax
import jax.numpy as jnp
from jax import lax
from jax.experimental import pallas as pl
from jax.experimental.pallas import tpu as pltpu
from jax.sharding import PartitionSpec as P

HEAD = 64
VDIM = 128
TOP = 2


eps = 1e-05
alpha_act = 1.702
limit_act = 7.0
negative = -1e30


def clamped_unit(gate, up):
    capped = jnp.minimum(gate, limit_act)
    linear = jnp.clip(up, -limit_act, limit_act)
    return capped * jax.nn.sigmoid(alpha_act * capped) * (linear + 1.0)


def hidden_rows(inputs, gate_matrix, up_matrix):
    gate = jnp.dot(inputs, gate_matrix, preferred_element_type=jnp.float32)
    up = jnp.dot(inputs, up_matrix, preferred_element_type=jnp.float32)
    return clamped_unit(gate, up).astype(jnp.bfloat16)


def pick_rows(table, owner):
    valid = owner < table.shape[0]
    chosen = jnp.take(table, jnp.minimum(owner, table.shape[0] - 1), axis=0)
    return jnp.where(valid[:, None], chosen, jnp.zeros_like(chosen))


def mixer(queries_a, queries_b, keys_a, keys_b, values, lambdas, head_gain, w_out):
    tokens = queries_a.shape[0]
    local_heads = lambdas.shape[0]
    kv_local = keys_a.shape[1] // HEAD
    group = local_heads // kv_local
    scale = HEAD ** (-0.5)
    query_pos = lax.axis_index("ep") * tokens + jnp.arange(tokens, dtype=jnp.int32)
    grouped_a = queries_a.reshape(tokens, kv_local, group, HEAD)
    grouped_b = queries_b.reshape(tokens, kv_local, group, HEAD)
    lowest = jnp.full((kv_local, group, tokens), negative, jnp.float32)
    nothing = jnp.zeros((kv_local, group, tokens), jnp.float32)
    blank = jnp.zeros((kv_local, group, tokens, VDIM), jnp.float32)

    def one_map(grouped, keys, value_rows, visible, state):
        peak, total, accum = state
        scores = (
            jnp.einsum("rgjd,ngd->gjrn", grouped, keys, preferred_element_type=jnp.float32) * scale
        )
        scores = jnp.where(visible, scores, negative)
        new_peak = jnp.maximum(peak, jnp.max(scores, axis=-1))
        expo = jnp.where(visible, jnp.exp(scores - new_peak[..., None]), 0.0)
        total = jnp.sum(expo, axis=-1)
        accum = jnp.einsum(
            "gjrn,ngv->gjrv",
            expo.astype(jnp.bfloat16),
            value_rows,
            preferred_element_type=jnp.float32,
        )
        return (new_peak, total, accum)

    initial = (lowest, nothing, blank, lowest, nothing, blank)
    piece_a = lax.all_gather(keys_a, "ep", axis=0, tiled=True)
    piece_b = lax.all_gather(keys_b, "ep", axis=0, tiled=True)
    piece_v = lax.all_gather(values, "ep", axis=0, tiled=True)
    count = piece_a.shape[0]

    def visit(state):
        key_pos = jnp.arange(count, dtype=jnp.int32)
        visible = key_pos[None, :] <= query_pos[:, None]
        value_rows = piece_v.reshape(count, kv_local, VDIM)
        first = one_map(
            grouped_a, piece_a.reshape(count, kv_local, HEAD), value_rows, visible, state[:3]
        )
        second = one_map(
            grouped_b, piece_b.reshape(count, kv_local, HEAD), value_rows, visible, state[3:]
        )
        return first + second

    result = lax.cond(jnp.int32(0) <= query_pos[tokens - 1], visit, lambda state: state, initial)
    mixed_a = result[2] / result[1][..., None]
    mixed_b = result[5] / result[4][..., None]
    diff = mixed_a - lambdas.reshape(kv_local, group, 1, 1) * mixed_b
    heads_out = (
        diff * lax.rsqrt(jnp.mean(diff * diff, axis=-1, keepdims=True) + eps) * head_gain
    ).astype(jnp.bfloat16)
    weights_out = w_out.reshape(kv_local, group, VDIM, w_out.shape[1])
    return lax.psum_scatter(
        jnp.einsum(
            "gjrv,gjvd->rd", heads_out, weights_out, preferred_element_type=jnp.float32
        ).astype(jnp.bfloat16),
        "tp",
        scatter_dimension=0,
        tiled=True,
    )


def experts(moe_tokens, moe_gain, routes, route_weights, w_gate, w_up, w_down):
    tok_rows, width = moe_tokens.shape
    n_experts = lax.axis_size("ep") * w_gate.shape[0]
    capacity = max(2, 3 * tok_rows * TOP // (2 * n_experts))
    inputs = moe_tokens.astype(jnp.float32)
    normed = (
        inputs * lax.rsqrt(jnp.mean(inputs * inputs, axis=-1, keepdims=True) + eps) * moe_gain
    ).astype(jnp.bfloat16)
    chosen = routes.reshape(-1)
    member = (chosen[:, None] == jnp.arange(n_experts, dtype=jnp.int32)[None, :]).astype(jnp.int32)
    order_in = jnp.sum(jnp.cumsum(member, axis=0) * member, axis=1) - 1
    slot_ids = chosen * capacity + order_in
    owner = (
        jnp.full((n_experts * capacity,), tok_rows, jnp.int32)
        .at[slot_ids]
        .set(jnp.arange(tok_rows * TOP, dtype=jnp.int32) // TOP)
    )
    outgoing = pick_rows(normed, owner).reshape(n_experts, capacity, width)
    arrived = lax.all_to_all(outgoing, "ep", split_axis=0, concat_axis=1, tiled=True).reshape(
        -1, width
    )
    hidden = hidden_rows(lax.all_gather(arrived, "tp", axis=0, tiled=True), w_gate[0], w_up[0])
    expert_out = lax.psum_scatter(
        jnp.dot(hidden, w_down[0], preferred_element_type=jnp.float32).astype(jnp.bfloat16),
        "tp",
        scatter_dimension=0,
        tiled=True,
    )
    returned = lax.all_to_all(
        expert_out.reshape(-1, capacity, width), "ep", split_axis=0, concat_axis=0, tiled=True
    )
    picked = jnp.take(returned.reshape(-1, width), slot_ids, axis=0).reshape(tok_rows, TOP, width)
    return jnp.sum(picked.astype(jnp.float32) * route_weights[:, :, None], axis=1).astype(
        jnp.bfloat16
    )


def body(
    queries_a,
    queries_b,
    keys_a,
    keys_b,
    values,
    lambdas,
    head_gain,
    w_out,
    moe_tokens,
    moe_gain,
    routes,
    route_weights,
    w_gate,
    w_up,
    w_down,
):
    mixer_out = mixer(queries_a, queries_b, keys_a, keys_b, values, lambdas, head_gain, w_out)
    moe_out = experts(moe_tokens, moe_gain, routes, route_weights, w_gate, w_up, w_down)
    return (mixer_out, moe_out)


MESH = pl.DeviceIdType.MESH
OUT, CORE, ACROSS, CORE_ACROSS, PART, PAIR, SUMS, BACK, KV_Z, KV_Y, MIX = range(11)


def xor(first, second, limit):
    total, bit = 0, 1
    while bit < limit:
        total = total + (first // bit + second // bit) % 2 * bit
        bit *= 2
    return total


def exchange(
    n, moe_tokens, gain_in, routes_in, weights_in, queries_a_in, queries_b_in, head_gain_in, lambdas_in,
    keys_a, keys_b, values, w_gate, w_up, w_down, w_out,
    moe_out, mixer_out,
    tokens_in, moe_gain, routes, route_weights, queries_a, queries_b, head_gain, lambdas,
    ret, outgoing, weigh, rows, parts, part_in, pair_in, sums_in, sums, final, hidden, gate_v, up_v, down_v, out_v,
    kv_all, heads, shares, mix_part, mix_pair, mix_in, mix_sum, send, recv, local,
):
    me = lax.axis_index("ep")
    tp = lax.axis_index("tp")
    core = tp + 1 - 2 * (tp % 2)
    across = tp + 2 - 4 * (tp // 2)
    diagonal = core + 2 - 4 * (core // 2)
    floor, lane = me // 2, me % 2
    floors = n // 2
    cap, width = outgoing.shape[1:]
    units = hidden.shape[1]
    flat = 4 * cap
    tokens = kv_all.shape[1]

    def mask_of(k):
        far = k // 2
        return 2 * ((far + 1) % 3 + 1) * ((far + 3) // 4) + k % 2

    def partner(k):
        return xor(me, mask_of(k), n)

    def copy(kind, k, source, target, device):
        return pltpu.make_async_remote_copy(
            src_ref=source,
            dst_ref=target,
            send_sem=send.at[kind, k],
            recv_sem=recv.at[kind, k],
            device_id=device,
            device_id_type=MESH,
        )

    def out_copy(k):
        return copy(OUT, k, outgoing.at[partner(k)], rows.at[k, 0], {"ep": partner(k)})

    def core_copy(k):
        return copy(CORE, k, rows.at[k, 0], rows.at[k, 1], {"tp": core})

    def across_copy(k):
        return copy(ACROSS, k, rows.at[k, 0], rows.at[k, 2], {"tp": across})

    def core_across_copy(k):
        return copy(CORE_ACROSS, k, rows.at[k, 2], rows.at[k, 3], {"tp": core})

    def part_copy(k):
        return copy(PART, k, parts.at[k, 1], part_in.at[k], {"tp": core})

    def pair_copy(k):
        return copy(PAIR, k, parts.at[k, 3], pair_in.at[k], {"tp": core})

    def sums_copy(k):
        return copy(SUMS, k, sums.at[k], sums_in.at[k], {"tp": across})

    def back_copy(k):
        return copy(BACK, k, final.at[k], ret.at[me], {"ep": partner(k)})

    def kv_z_copy(stage):
        block = kv_all.at[2 * (floor - stage + 1) + lane]
        return copy(KV_Z, stage, block, block, {"ep": me + 2})

    def kv_y_copy(stage):
        block = kv_all.at[2 * (floor - stage) + lane]
        return copy(KV_Y, stage, block, block, {"ep": me + 1 - 2 * lane})

    mix_part_copy = copy(MIX, 0, shares.at[core], mix_part, {"tp": core})
    mix_pair_copy = copy(MIX, 1, shares.at[diagonal], mix_pair, {"tp": core})
    mix_sum_copy = copy(MIX, 2, mix_sum, mix_in, {"tp": across})

    local_heads = heads.shape[1] // VDIM
    kv_local = kv_all.shape[2] // (2 * HEAD + VDIM)
    span = kv_local * HEAD

    def one_map(queries, head, offset):
        g = head // (local_heads // kv_local)
        count = n * tokens
        first = offset + g * HEAD
        keys = kv_all[:, :, first : first + HEAD].reshape(count, HEAD)
        first = 2 * span + g * VDIM
        value_rows = kv_all[:, :, first : first + VDIM].reshape(count, VDIM)
        scores = lax.dot_general(
            queries[:, head * HEAD : (head + 1) * HEAD],
            keys,
            (((1,), (1,)), ((), ())),
            preferred_element_type=jnp.float32,
        ) * HEAD ** (-0.5)
        query_pos = me * tokens + lax.broadcasted_iota(jnp.int32, scores.shape, 0)
        key_pos = lax.broadcasted_iota(jnp.int32, scores.shape, 1)
        scores = jnp.where(key_pos <= query_pos, scores, negative)
        expo = jnp.exp(scores - jnp.max(scores, axis=1, keepdims=True))
        total = jnp.sum(expo, axis=1, keepdims=True)
        mixed = jnp.dot(
            expo.astype(jnp.bfloat16), value_rows, preferred_element_type=jnp.float32
        )
        return mixed / total

    def attend(head):
        diff = one_map(queries_a, head, 0) - lambdas[head] * one_map(queries_b, head, span)
        norm = lax.rsqrt(jnp.mean(diff * diff, axis=1, keepdims=True) + eps)
        heads[:, head * VDIM : (head + 1) * VDIM] = (diff * norm * head_gain[...]).astype(
            jnp.bfloat16
        )

    def forward(k):
        core_copy(k).start()
        across_copy(k).start()

    def relay(k):
        across_copy(k).wait_recv()
        core_across_copy(k).start()

    def send_sums(k):
        pair_copy(k).wait_recv()
        sums[k] = (
            parts[k, 2].astype(jnp.float32) + pair_in[k].astype(jnp.float32)
        ).astype(jnp.bfloat16)
        sums_copy(k).start()

    def finish(k):
        part_copy(k).wait_recv()
        sums_copy(k).wait_recv()
        return (
            parts[k, 0].astype(jnp.float32)
            + part_in[k].astype(jnp.float32)
            + sums_in[k].astype(jnp.float32)
        ).astype(jnp.bfloat16)

    def send_back(k):
        final[k] = finish(k)
        back_copy(k).start()

    def feed(k):
        core_copy(k).wait_recv()
        core_across_copy(k).wait_recv()
        inputs = rows[k].reshape(flat, width)
        step = min(256, units)
        for first in range(0, units, step):
            gate = jnp.dot(
                inputs, gate_v[:, first : first + step], preferred_element_type=jnp.float32
            )
            up = jnp.dot(
                inputs, up_v[:, first : first + step], preferred_element_type=jnp.float32
            )
            hidden[:, first : first + step] = clamped_unit(gate, up).astype(jnp.bfloat16)
        for first in range(0, width, 256):
            piece = jnp.dot(
                hidden[...], down_v[:, first : first + 256], preferred_element_type=jnp.float32
            )
            parts[k, :, :, first : first + 256] = piece.astype(jnp.bfloat16).reshape(
                4, cap, 256
            )
        pair_copy(k).start()
        part_copy(k).start()

    barrier = pltpu.get_barrier_semaphore()
    for shift in range(1, n):
        pl.semaphore_signal(
            barrier, inc=1, device_id={"ep": (me + shift) % n}, device_id_type=MESH
        )
    for shift in range(1, 4):
        pl.semaphore_signal(
            barrier, inc=1, device_id={"tp": (tp + shift) % 4}, device_id_type=MESH
        )

    pairs = [
        (moe_tokens, tokens_in), (gain_in, moe_gain), (routes_in, routes),
        (keys_a, kv_all.at[me, :, 0:span]), (keys_b, kv_all.at[me, :, span : 2 * span]),
        (values, kv_all.at[me, :, 2 * span :]), (weights_in, route_weights),
        (w_gate, gate_v), (w_up, up_v), (w_down, down_v), (w_out, out_v),
        (queries_a_in, queries_a), (queries_b_in, queries_b), (head_gain_in, head_gain),
        (lambdas_in, lambdas),
    ]
    loads = [
        pltpu.make_async_copy(source, target, local.at[i])
        for i, (source, target) in enumerate(pairs)
    ]
    for load in loads:
        load.start()
    for load in loads[:3]:
        load.wait()

    inputs = tokens_in[...].astype(jnp.float32)
    normed = (
        inputs
        * lax.rsqrt(jnp.mean(inputs * inputs, axis=1, keepdims=True) + eps)
        * moe_gain[...]
    ).astype(jnp.bfloat16)
    count = tokens_in.shape[0]
    expert = lax.broadcasted_iota(jnp.int32, (n, count), 0)
    named = [routes[k : k + 1, :] == expert for k in range(TOP)]
    member = named[0]
    for k in range(1, TOP):
        member = member | named[k]
    earlier = lax.broadcasted_iota(jnp.int32, (count, count), 0) < lax.broadcasted_iota(
        jnp.int32, (count, count), 1
    )
    place = jnp.dot(
        jnp.where(member, 1.0, 0.0).astype(jnp.bfloat16),
        jnp.where(earlier, 1.0, 0.0).astype(jnp.bfloat16),
        preferred_element_type=jnp.float32,
    )
    position = lax.broadcasted_iota(jnp.int32, (cap, count), 0).astype(jnp.float32)
    slot = jnp.where(member, place, -1.0)
    for e in range(n):
        pick = jnp.where(slot[e : e + 1, :] == position, 1.0, 0.0).astype(jnp.bfloat16)
        outgoing[e] = jnp.dot(pick, normed, preferred_element_type=jnp.float32).astype(
            jnp.bfloat16
        )
    rows[0, 0] = outgoing[me]
    pl.semaphore_wait(barrier, n + 2)

    forward(0)
    for k in range(1, n // 2):
        out_copy(k).start()
    for load in loads[3:7]:
        load.wait()

    @pl.when(floor < floors - 1)
    def _():
        kv_z_copy(1).start()

    for k in range(n // 2, n):
        out_copy(k).start()
    kv_y_copy(0).start()

    for other in range(1, floors):

        @pl.when(floor < other)
        def _():
            for side in range(2):
                kv_all[2 * other + side] = jnp.zeros(kv_all.shape[1:], jnp.bfloat16)

    share = route_weights[...]
    scale = jnp.where(named[0], share[0:1, :], 0.0)
    for k in range(1, TOP):
        scale = scale + jnp.where(named[k], share[k : k + 1, :], 0.0)
    table = jnp.concatenate(
        [
            jnp.where(slot[e : e + 1, :] == position, scale[e : e + 1, :], 0.0)
            for e in range(n)
        ],
        axis=0,
    ).T
    high = table.astype(jnp.bfloat16)
    weigh[0] = high
    weigh[1] = (table - high.astype(jnp.float32)).astype(jnp.bfloat16)
    for load in loads[7:]:
        load.wait()

    def kv_next(stage):
        @pl.when(floor >= stage)
        def _():
            kv_z_copy(stage).wait_recv()
            kv_y_copy(stage).start()
            if stage < floors - 1:

                @pl.when(floor < floors - 1)
                def _():
                    kv_z_copy(stage + 1).start()

    @pl.loop(0, n)
    def _(k):
        @pl.when((k >= 2) & (k < 4))
        def _():
            send_sums(k - 1)

        @pl.when(k + 1 < n)
        def _():
            out_copy(k + 1).wait_recv()
            forward(k + 1)

        @pl.when(k == 4)
        def _():
            send_sums(3)
            send_back(1)
            kv_next(1)

        @pl.when(k == 5)
        def _():
            send_back(2)

        @pl.when(k == 6)
        def _():
            send_sums(4)
            send_back(3)
            kv_next(2)

        @pl.when(k == 7)
        def _():
            send_sums(6)
            kv_next(3)

        relay(k)
        feed(k)

    send_sums(7)
    send_back(4)
    send_sums(5)
    for stage in range(floors):

        @pl.when(floor >= stage)
        def _():
            kv_y_copy(stage).wait_recv()

    for head in range(local_heads):
        attend(head)
    send_back(6)
    for first in range(0, width, 256):
        piece = jnp.dot(
            heads[...], out_v[:, first : first + 256], preferred_element_type=jnp.float32
        )
        shares[:, :, first : first + 256] = piece.astype(jnp.bfloat16).reshape(
            4, tokens // 4, 256
        )
    mix_pair_copy.start()
    mix_part_copy.start()
    mix_pair_copy.wait_recv()
    mix_sum[...] = (
        shares[across].astype(jnp.float32) + mix_pair[...].astype(jnp.float32)
    ).astype(jnp.bfloat16)
    mix_sum_copy.start()
    send_sums(0)
    send_back(7)
    send_back(5)
    ret[me] = finish(0)

    @pl.loop(1, n)
    def _(k):
        back_copy(k).wait_recv()

    for first in range(0, width, 256):
        table = ret[:, :, first : first + 256].reshape(n * cap, 256)
        total = jnp.dot(weigh[0], table, preferred_element_type=jnp.float32) + jnp.dot(
            weigh[1], table, preferred_element_type=jnp.float32
        )
        moe_out[:, first : first + 256] = total.astype(jnp.bfloat16)

    mix_part_copy.wait_recv()
    mix_sum_copy.wait_recv()
    mixer_out[...] = (
        shares[tp].astype(jnp.float32)
        + mix_part[...].astype(jnp.float32)
        + mix_in[...].astype(jnp.float32)
    ).astype(jnp.bfloat16)

    for made in (mix_part_copy, mix_pair_copy, mix_sum_copy):
        made.wait_send()
    for stage in range(1, floors):

        @pl.when((floor >= stage - 1) & (floor < floors - 1))
        def _():
            kv_z_copy(stage).wait_send()

    for stage in range(floors):

        @pl.when(floor >= stage)
        def _():
            kv_y_copy(stage).wait_send()

    @pl.loop(0, n)
    def _(k):
        for made in (core_copy, across_copy, core_across_copy, part_copy, pair_copy, sums_copy):
            made(k).wait_send()

        @pl.when(k >= 1)
        def _():
            out_copy(k).wait_send()
            back_copy(k).wait_send()


def run_exchange(
    n, cap, tokens_in, moe_gain, routes, route_weights, queries_a, queries_b, head_gain,
    lambdas, keys_a, keys_b, values, w_gate, w_up, w_down, w_out,
):
    count, width = tokens_in.shape
    units = w_gate.shape[1]
    block = (n, cap, width)
    tokens = keys_a.shape[0]
    kv_width = keys_a.shape[1] + keys_b.shape[1] + values.shape[1]
    quarter = (tokens // 4, width)
    vmem = pl.BlockSpec(memory_space=pltpu.VMEM)
    hbm = pl.BlockSpec(memory_space=pltpu.HBM)
    call = pl.pallas_call(
        functools.partial(exchange, n),
        out_shape=(
            pltpu.VMEM((count, width), jnp.bfloat16),
            pltpu.VMEM(quarter, jnp.bfloat16),
        ),
        in_specs=[hbm] * 15,
        out_specs=(vmem, vmem),
        scratch_shapes=[
            pltpu.VMEM(tokens_in.shape, jnp.bfloat16),
            pltpu.VMEM((1, width), jnp.float32),
            pltpu.VMEM((TOP, count), jnp.int32),
            pltpu.VMEM((TOP, count), jnp.float32),
            pltpu.VMEM(queries_a.shape, jnp.bfloat16),
            pltpu.VMEM(queries_b.shape, jnp.bfloat16),
            pltpu.VMEM((1, VDIM), jnp.float32),
            pltpu.SMEM(lambdas.shape, jnp.float32),
            pltpu.VMEM(block, jnp.bfloat16),
            pltpu.VMEM(block, jnp.bfloat16),
            pltpu.VMEM((2, count, n * cap), jnp.bfloat16),
            pltpu.VMEM((n, 4, cap, width), jnp.bfloat16),
            pltpu.VMEM((n, 4, cap, width), jnp.bfloat16),
            pltpu.VMEM(block, jnp.bfloat16),
            pltpu.VMEM(block, jnp.bfloat16),
            pltpu.VMEM(block, jnp.bfloat16),
            pltpu.VMEM(block, jnp.bfloat16),
            pltpu.VMEM(block, jnp.bfloat16),
            pltpu.VMEM((4 * cap, units), jnp.bfloat16),
            pltpu.VMEM(w_gate.shape, jnp.bfloat16),
            pltpu.VMEM(w_up.shape, jnp.bfloat16),
            pltpu.VMEM(w_down.shape, jnp.bfloat16),
            pltpu.VMEM(w_out.shape, jnp.bfloat16),
            pltpu.VMEM((n, tokens, kv_width), jnp.bfloat16),
            pltpu.VMEM((tokens, w_out.shape[0]), jnp.bfloat16),
            pltpu.VMEM((4,) + quarter, jnp.bfloat16),
            pltpu.VMEM(quarter, jnp.bfloat16),
            pltpu.VMEM(quarter, jnp.bfloat16),
            pltpu.VMEM(quarter, jnp.bfloat16),
            pltpu.VMEM(quarter, jnp.bfloat16),
            pltpu.SemaphoreType.DMA((11, n)),
            pltpu.SemaphoreType.DMA((11, n)),
            pltpu.SemaphoreType.DMA((15,)),
        ],
        compiler_params=pltpu.CompilerParams(
            collective_id=0, has_side_effects=True, vmem_limit_bytes=48 * 2**20
        ),
        name="exchange",
    )
    operands = (
        tokens_in, moe_gain.reshape(1, -1), routes.T, route_weights.T,
        queries_a, queries_b, head_gain.reshape(1, -1), lambdas,
        keys_a, keys_b, values, w_gate, w_up, w_down, w_out,
    )
    return call(*[pltpu.with_memory_space_constraint(x, pltpu.HBM) for x in operands])


def fast_body(
    queries_a, queries_b, keys_a, keys_b, values, lambdas, head_gain, w_out,
    moe_tokens, moe_gain, routes, route_weights, w_gate, w_up, w_down,
):
    n = lax.axis_size("ep")
    cap = 3 * moe_tokens.shape[0] * TOP // (2 * n)
    moe_out, mixer_out = run_exchange(
        n, cap, moe_tokens, moe_gain, routes, route_weights, queries_a, queries_b,
        head_gain, lambdas, keys_a, keys_b, values, w_gate[0], w_up[0], w_down[0], w_out,
    )
    return (mixer_out, moe_out)


def whole_body(*args):
    n, n_tp = lax.axis_size("ep"), lax.axis_size("tp")
    tok_rows, w_gate = args[8].shape[0], args[12]
    cap = 3 * tok_rows * TOP // (2 * n)
    if w_gate.shape[0] == 1 and n_tp == 4 and n == 8 and cap % 16 == 0:
        return fast_body(*args)
    return body(*args)


def solution(mesh):
    return jax.shard_map(
        whole_body,
        mesh=mesh,
        in_specs=(
            P("ep", "tp"),
            P("ep", "tp"),
            P("ep", "tp"),
            P("ep", "tp"),
            P("ep", "tp"),
            P("tp"),
            P(),
            P("tp", None),
            P(("ep", "tp"), None),
            P(),
            P(("ep", "tp"), None),
            P(("ep", "tp"), None),
            P("ep", None, "tp"),
            P("ep", None, "tp"),
            P("ep", "tp", None),
        ),
        out_specs=(P(("ep", "tp"), None), P(("ep", "tp"), None)),
        check_vma=False,
    )
```

```python
import functools

import jax
import jax.numpy as jnp
from jax import lax
from jax.experimental import pallas as pl
from jax.experimental.pallas import tpu as pltpu
from jax.sharding import PartitionSpec as P

HEAD = 64
VDIM = 128
TOP = 2


eps = 1e-05
alpha_act = 1.702
limit_act = 7.0
negative = -1e30


def clamped_unit(gate, up):
    capped = jnp.minimum(gate, limit_act)
    linear = jnp.clip(up, -limit_act, limit_act)
    return capped * jax.nn.sigmoid(alpha_act * capped) * (linear + 1.0)


def hidden_rows(inputs, gate_matrix, up_matrix):
    gate = jnp.dot(inputs, gate_matrix, preferred_element_type=jnp.float32)
    up = jnp.dot(inputs, up_matrix, preferred_element_type=jnp.float32)
    return clamped_unit(gate, up).astype(jnp.bfloat16)


def pick_rows(table, owner):
    valid = owner < table.shape[0]
    chosen = jnp.take(table, jnp.minimum(owner, table.shape[0] - 1), axis=0)
    return jnp.where(valid[:, None], chosen, jnp.zeros_like(chosen))


def mixer(queries_a, queries_b, keys_a, keys_b, values, lambdas, head_gain, w_out):
    tokens = queries_a.shape[0]
    local_heads = lambdas.shape[0]
    kv_local = keys_a.shape[1] // HEAD
    group = local_heads // kv_local
    scale = HEAD ** (-0.5)
    query_pos = lax.axis_index("ep") * tokens + jnp.arange(tokens, dtype=jnp.int32)
    grouped_a = queries_a.reshape(tokens, kv_local, group, HEAD)
    grouped_b = queries_b.reshape(tokens, kv_local, group, HEAD)
    lowest = jnp.full((kv_local, group, tokens), negative, jnp.float32)
    nothing = jnp.zeros((kv_local, group, tokens), jnp.float32)
    blank = jnp.zeros((kv_local, group, tokens, VDIM), jnp.float32)

    def one_map(grouped, keys, value_rows, visible, state):
        peak, total, accum = state
        scores = (
            jnp.einsum("rgjd,ngd->gjrn", grouped, keys, preferred_element_type=jnp.float32) * scale
        )
        scores = jnp.where(visible, scores, negative)
        new_peak = jnp.maximum(peak, jnp.max(scores, axis=-1))
        expo = jnp.where(visible, jnp.exp(scores - new_peak[..., None]), 0.0)
        total = jnp.sum(expo, axis=-1)
        accum = jnp.einsum(
            "gjrn,ngv->gjrv",
            expo.astype(jnp.bfloat16),
            value_rows,
            preferred_element_type=jnp.float32,
        )
        return (new_peak, total, accum)

    initial = (lowest, nothing, blank, lowest, nothing, blank)
    piece_a = lax.all_gather(keys_a, "ep", axis=0, tiled=True)
    piece_b = lax.all_gather(keys_b, "ep", axis=0, tiled=True)
    piece_v = lax.all_gather(values, "ep", axis=0, tiled=True)
    count = piece_a.shape[0]

    def visit(state):
        key_pos = jnp.arange(count, dtype=jnp.int32)
        visible = key_pos[None, :] <= query_pos[:, None]
        value_rows = piece_v.reshape(count, kv_local, VDIM)
        first = one_map(
            grouped_a, piece_a.reshape(count, kv_local, HEAD), value_rows, visible, state[:3]
        )
        second = one_map(
            grouped_b, piece_b.reshape(count, kv_local, HEAD), value_rows, visible, state[3:]
        )
        return first + second

    result = lax.cond(jnp.int32(0) <= query_pos[tokens - 1], visit, lambda state: state, initial)
    mixed_a = result[2] / result[1][..., None]
    mixed_b = result[5] / result[4][..., None]
    diff = mixed_a - lambdas.reshape(kv_local, group, 1, 1) * mixed_b
    heads_out = (
        diff * lax.rsqrt(jnp.mean(diff * diff, axis=-1, keepdims=True) + eps) * head_gain
    ).astype(jnp.bfloat16)
    weights_out = w_out.reshape(kv_local, group, VDIM, w_out.shape[1])
    return lax.psum_scatter(
        jnp.einsum(
            "gjrv,gjvd->rd", heads_out, weights_out, preferred_element_type=jnp.float32
        ).astype(jnp.bfloat16),
        "tp",
        scatter_dimension=0,
        tiled=True,
    )


def experts(moe_tokens, moe_gain, routes, route_weights, w_gate, w_up, w_down):
    tok_rows, width = moe_tokens.shape
    n_experts = lax.axis_size("ep") * w_gate.shape[0]
    capacity = max(2, 3 * tok_rows * TOP // (2 * n_experts))
    inputs = moe_tokens.astype(jnp.float32)
    normed = (
        inputs * lax.rsqrt(jnp.mean(inputs * inputs, axis=-1, keepdims=True) + eps) * moe_gain
    ).astype(jnp.bfloat16)
    chosen = routes.reshape(-1)
    member = (chosen[:, None] == jnp.arange(n_experts, dtype=jnp.int32)[None, :]).astype(jnp.int32)
    order_in = jnp.sum(jnp.cumsum(member, axis=0) * member, axis=1) - 1
    slot_ids = chosen * capacity + order_in
    owner = (
        jnp.full((n_experts * capacity,), tok_rows, jnp.int32)
        .at[slot_ids]
        .set(jnp.arange(tok_rows * TOP, dtype=jnp.int32) // TOP)
    )
    outgoing = pick_rows(normed, owner).reshape(n_experts, capacity, width)
    arrived = lax.all_to_all(outgoing, "ep", split_axis=0, concat_axis=1, tiled=True).reshape(
        -1, width
    )
    hidden = hidden_rows(lax.all_gather(arrived, "tp", axis=0, tiled=True), w_gate[0], w_up[0])
    expert_out = lax.psum_scatter(
        jnp.dot(hidden, w_down[0], preferred_element_type=jnp.float32).astype(jnp.bfloat16),
        "tp",
        scatter_dimension=0,
        tiled=True,
    )
    returned = lax.all_to_all(
        expert_out.reshape(-1, capacity, width), "ep", split_axis=0, concat_axis=0, tiled=True
    )
    picked = jnp.take(returned.reshape(-1, width), slot_ids, axis=0).reshape(tok_rows, TOP, width)
    return jnp.sum(picked.astype(jnp.float32) * route_weights[:, :, None], axis=1).astype(
        jnp.bfloat16
    )


def body(
    queries_a,
    queries_b,
    keys_a,
    keys_b,
    values,
    lambdas,
    head_gain,
    w_out,
    moe_tokens,
    moe_gain,
    routes,
    route_weights,
    w_gate,
    w_up,
    w_down,
):
    mixer_out = mixer(queries_a, queries_b, keys_a, keys_b, values, lambdas, head_gain, w_out)
    moe_out = experts(moe_tokens, moe_gain, routes, route_weights, w_gate, w_up, w_down)
    return (mixer_out, moe_out)


MESH = pl.DeviceIdType.MESH
OUT, ACROSS, CORE, PAIR, PART, KV_Z, KV_Y, MIX, BACK, RELAYS, HALVES, TRIPS = range(12)


def xor(first, second, limit):
    total, bit = 0, 1
    while bit < limit:
        total = total + (first // bit + second // bit) % 2 * bit
        bit *= 2
    return total


def exchange(
    n, moe_tokens, gain_in, routes_in, weights_in, queries_a_in, queries_b_in, head_gain_in, lambdas_in,
    keys_a, keys_b, values, w_gate, w_up, w_down, w_out,
    moe_out, mixer_out,
    tokens_in, moe_gain, routes, route_weights, queries_a, queries_b, head_gain, lambdas,
    ret, outgoing, weigh, rows, parts, part_in, pair_in, sums, final, hidden, gate_v, up_v, down_v, out_v,
    kv_all, heads, shares, mix_part, mix_pair, mix_in, mix_sum, send, recv, local,
):
    me = lax.axis_index("ep")
    tp = lax.axis_index("tp")
    core = tp + 1 - 2 * (tp % 2)
    across = tp + 2 - 4 * (tp // 2)
    diagonal = core + 2 - 4 * (core // 2)
    floor, lane = me // 2, me % 2
    floors = n // 2
    cap, width = outgoing.shape[1:]
    units = hidden.shape[1]
    flat = 4 * cap
    tokens = kv_all.shape[1]

    inner = (floor + 1) // 2 % 2

    def order(step):
        turn = step // 2
        return step + inner * (2 * (turn // 2 + 2 * (turn % 2)) + step % 2 - step)

    def partner(k):
        return xor(me, k, n)

    def place_of(kind, k):
        return n * kind + k if kind < KV_Z else 5 * n + 4 * (kind - KV_Z) + k

    def sent_by(kind, k):
        return kind - BACK if kind > BACK else 3 + 4 * (kind - KV_Z) + k

    def copy(kind, k, group, source, target, device):
        return pltpu.make_async_remote_copy(
            src_ref=source,
            dst_ref=target,
            send_sem=send.at[sent_by(group, k)],
            recv_sem=recv.at[place_of(kind, k)],
            device_id=device,
            device_id_type=MESH,
        )

    def out_copy(k):
        return copy(OUT, k, TRIPS, outgoing.at[partner(k)], rows.at[k, 0], {"ep": partner(k)})

    def core_copy(k):
        return copy(CORE, k, RELAYS, rows.at[k, 0], rows.at[k, 1], {"tp": core})

    def across_copy(k):
        return copy(ACROSS, k, RELAYS, rows.at[k, 0], rows.at[k, 2], {"tp": across})

    def core_across_copy(k):
        return copy(CORE, k, RELAYS, rows.at[k, 2], rows.at[k, 3], {"tp": core})

    def both_core_copies(k):
        return copy(CORE, k, RELAYS, rows.at[k, 0:2], rows.at[k, 2:4], {"tp": core})

    def part_copy(k):
        return copy(PART, k, HALVES, parts.at[k, 1], part_in.at[0, k], {"tp": core})

    def pair_copy(k):
        return copy(PAIR, k, HALVES, parts.at[k, 3], pair_in.at[k], {"tp": core})

    def sums_copy(k):
        return copy(PART, k, RELAYS, sums.at[k], part_in.at[1, k], {"tp": across})

    def part_and_sums(k):
        return copy(PART, k, RELAYS, rows.at[k, 0:2], part_in.at[:, k], {"tp": across})

    def back_copy(k):
        return copy(BACK, 0, TRIPS, final.at[k], ret.at[me], {"ep": partner(k)})

    def all_back():
        return copy(BACK, 0, TRIPS, final.at[0 : n - 1], ret.at[0 : n - 1], {"tp": core})

    def all_sent():
        return [
            copy(OUT, 0, RELAYS, rows, rows, {"tp": core}),
            copy(OUT, 0, HALVES, rows.at[:, 0:2], rows.at[:, 0:2], {"tp": core}),
            copy(OUT, 0, TRIPS, rows.at[0 : n - 1, 0:2], rows.at[0 : n - 1, 0:2], {"tp": core}),
        ]

    def kv_z_copy(stage):
        block = kv_all.at[2 * (floor - stage + 1) + lane]
        return copy(KV_Z, stage, KV_Z, block, block, {"ep": me + 2})

    def kv_y_copy(stage):
        block = kv_all.at[2 * (floor - stage) + lane]
        return copy(KV_Y, stage, KV_Y, block, block, {"ep": me + 1 - 2 * lane})

    mix_part_copy = copy(MIX, 0, MIX, shares.at[core], mix_part, {"tp": core})
    mix_pair_copy = copy(MIX, 1, MIX, shares.at[diagonal], mix_pair, {"tp": core})
    mix_sum_copy = copy(MIX, 2, MIX, mix_sum, mix_in, {"tp": across})

    local_heads = heads.shape[1] // VDIM
    kv_local = kv_all.shape[2] // (2 * HEAD + VDIM)
    span = kv_local * HEAD

    def one_map(queries, head, offset):
        g = head // (local_heads // kv_local)
        count = n * tokens
        first = offset + g * HEAD
        keys = kv_all[:, :, first : first + HEAD].reshape(count, HEAD)
        first = 2 * span + g * VDIM
        value_rows = kv_all[:, :, first : first + VDIM].reshape(count, VDIM)
        scores = lax.dot_general(
            queries[:, head * HEAD : (head + 1) * HEAD],
            keys,
            (((1,), (1,)), ((), ())),
            preferred_element_type=jnp.float32,
        ) * HEAD ** (-0.5)
        query_pos = me * tokens + lax.broadcasted_iota(jnp.int32, scores.shape, 0)
        key_pos = lax.broadcasted_iota(jnp.int32, scores.shape, 1)
        scores = jnp.where(key_pos <= query_pos, scores, negative)
        expo = jnp.exp(scores - jnp.max(scores, axis=1, keepdims=True))
        total = jnp.sum(expo, axis=1, keepdims=True)
        mixed = jnp.dot(
            expo.astype(jnp.bfloat16), value_rows, preferred_element_type=jnp.float32
        )
        return mixed / total

    def attend(head):
        diff = one_map(queries_a, head, 0) - lambdas[head] * one_map(queries_b, head, span)
        norm = lax.rsqrt(jnp.mean(diff * diff, axis=1, keepdims=True) + eps)
        heads[:, head * VDIM : (head + 1) * VDIM] = (diff * norm * head_gain[...]).astype(
            jnp.bfloat16
        )

    def forward(k):
        core_copy(k).start()
        across_copy(k).start()

    def relay(k):
        across_copy(k).wait_recv()
        core_across_copy(k).start()

    def send_sums(k):
        pair_copy(k).wait_recv()
        sums[k] = (
            parts[k, 2].astype(jnp.float32) + pair_in[k].astype(jnp.float32)
        ).astype(jnp.bfloat16)
        sums_copy(k).start()

    def finish(k):
        part_and_sums(k).wait_recv()
        return (
            parts[k, 0].astype(jnp.float32)
            + part_in[0, k].astype(jnp.float32)
            + part_in[1, k].astype(jnp.float32)
        ).astype(jnp.bfloat16)

    def send_back(k):
        final[k] = finish(k)
        back_copy(k).start()

    def feed(k):
        both_core_copies(k).wait_recv()
        inputs = rows[k].reshape(flat, width)
        step = min(256, units)
        for first in range(0, units, step):
            gate = jnp.dot(
                inputs, gate_v[:, first : first + step], preferred_element_type=jnp.float32
            )
            up = jnp.dot(
                inputs, up_v[:, first : first + step], preferred_element_type=jnp.float32
            )
            hidden[:, first : first + step] = clamped_unit(gate, up).astype(jnp.bfloat16)
        for first in range(0, width, 256):
            piece = jnp.dot(
                hidden[...], down_v[:, first : first + 256], preferred_element_type=jnp.float32
            )
            parts[k, :, :, first : first + 256] = piece.astype(jnp.bfloat16).reshape(
                4, cap, 256
            )
        pair_copy(k).start()
        part_copy(k).start()

    barrier = pltpu.get_barrier_semaphore()
    for shift in range(1, n):
        pl.semaphore_signal(
            barrier, inc=1, device_id={"ep": (me + shift) % n}, device_id_type=MESH
        )
    for shift in range(1, 4):
        pl.semaphore_signal(
            barrier, inc=1, device_id={"tp": (tp + shift) % 4}, device_id_type=MESH
        )

    pairs = [
        (moe_tokens, tokens_in), (gain_in, moe_gain), (routes_in, routes),
        (keys_a, kv_all.at[me, :, 0:span]), (keys_b, kv_all.at[me, :, span : 2 * span]),
        (values, kv_all.at[me, :, 2 * span :]), (weights_in, route_weights),
        (w_gate, gate_v), (w_up, up_v), (w_down, down_v), (w_out, out_v),
        (queries_a_in, queries_a), (queries_b_in, queries_b), (head_gain_in, head_gain),
        (lambdas_in, lambdas),
    ]
    loads = [
        pltpu.make_async_copy(source, target, local.at[i])
        for i, (source, target) in enumerate(pairs)
    ]
    for load in loads:
        load.start()
    for load in loads[:3]:
        load.wait()

    inputs = tokens_in[...].astype(jnp.float32)
    normed = (
        inputs
        * lax.rsqrt(jnp.mean(inputs * inputs, axis=1, keepdims=True) + eps)
        * moe_gain[...]
    ).astype(jnp.bfloat16)
    count = tokens_in.shape[0]
    expert = lax.broadcasted_iota(jnp.int32, (n, count), 0)
    named = [routes[k : k + 1, :] == expert for k in range(TOP)]
    member = named[0]
    for k in range(1, TOP):
        member = member | named[k]
    earlier = lax.broadcasted_iota(jnp.int32, (count, count), 0) < lax.broadcasted_iota(
        jnp.int32, (count, count), 1
    )
    place = jnp.dot(
        jnp.where(member, 1.0, 0.0).astype(jnp.bfloat16),
        jnp.where(earlier, 1.0, 0.0).astype(jnp.bfloat16),
        preferred_element_type=jnp.float32,
    )
    position = lax.broadcasted_iota(jnp.int32, (cap, count), 0).astype(jnp.float32)
    slot = jnp.where(member, place, -1.0)
    for e in range(n):
        pick = jnp.where(slot[e : e + 1, :] == position, 1.0, 0.0).astype(jnp.bfloat16)
        outgoing[e] = jnp.dot(pick, normed, preferred_element_type=jnp.float32).astype(
            jnp.bfloat16
        )
    rows[0, 0] = outgoing[me]
    pl.semaphore_wait(barrier, n + 2)

    forward(0)
    for k in (1, 4, 2):
        out_copy(k).start()

    for other in range(1, floors):

        @pl.when(floor < other)
        def _():
            for side in range(2):
                kv_all[2 * other + side] = jnp.zeros(kv_all.shape[1:], jnp.bfloat16)

    for load in loads[3:7]:
        load.wait()
    share = route_weights[...]
    scale = jnp.where(named[0], share[0:1, :], 0.0)
    for k in range(1, TOP):
        scale = scale + jnp.where(named[k], share[k : k + 1, :], 0.0)
    table = jnp.concatenate(
        [
            jnp.where(slot[e : e + 1, :] == position, scale[e : e + 1, :], 0.0)
            for e in range(n)
        ],
        axis=0,
    ).T
    high = table.astype(jnp.bfloat16)
    weigh[0] = high
    weigh[1] = (table - high.astype(jnp.float32)).astype(jnp.bfloat16)
    out_copy(5).start()
    for load in loads[7:]:
        load.wait()

    def kv_next(stage):
        @pl.when(floor >= stage)
        def _():
            kv_z_copy(stage).wait_recv()
            kv_y_copy(stage).start()
            if stage < floors - 1:

                @pl.when(floor < floors - 1)
                def _():
                    kv_z_copy(stage + 1).start()

    def pass_on(k):
        out_copy(k).wait_recv()
        forward(k)

    @pl.loop(0, n)
    def _(step):
        @pl.when(step == 3)
        def _():
            send_sums(1)

        @pl.when(step < 5)
        def _():
            pass_on(order(step + 1))

        for k in (6, 7):

            @pl.when(step == k - 2 + inner)
            def _():
                pass_on(k)

        for k in (4, 5):

            @pl.when(step == k + 2 - inner)
            def _():
                send_sums(k)

        @pl.when(step == 0)
        def _():
            out_copy(3).start()
            out_copy(6).start()

        @pl.when(step == 1)
        def _():
            out_copy(7).start()

        @pl.when(step == 2)
        def _():
            @pl.when(floor < floors - 1)
            def _():
                kv_z_copy(1).start()

            kv_y_copy(0).start()

        @pl.when(step == 5)
        def _():
            send_back(1)

        @pl.when(step == 6)
        def _():
            kv_next(1)

        @pl.when((step == 7) & (inner == 1))
        def _():
            send_sums(6)
            send_back(4)

        @pl.when(step == 7)
        def _():
            kv_next(2)

        relay(order(step))
        feed(order(step))

    @pl.when(inner == 0)
    def _():
        send_sums(6)

    send_sums(7)

    @pl.when(inner == 0)
    def _():
        send_back(4)

    send_back(5)
    send_sums(2)
    send_sums(3)
    kv_next(3)
    for stage in range(floors):

        @pl.when(floor >= stage)
        def _():
            kv_y_copy(stage).wait_recv()

    for head in range(local_heads):
        attend(head)
    send_back(6)
    for first in range(0, width, 256):
        piece = jnp.dot(
            heads[...], out_v[:, first : first + 256], preferred_element_type=jnp.float32
        )
        shares[:, :, first : first + 256] = piece.astype(jnp.bfloat16).reshape(
            4, tokens // 4, 256
        )
    mix_pair_copy.start()
    mix_part_copy.start()
    send_back(7)
    mix_pair_copy.wait_recv()
    mix_sum[...] = (
        shares[across].astype(jnp.float32) + mix_pair[...].astype(jnp.float32)
    ).astype(jnp.bfloat16)
    mix_sum_copy.start()
    send_sums(0)
    send_back(2)
    send_back(3)
    ret[me] = finish(0)

    all_back().wait_recv()
    for first in range(0, width, 256):
        table = ret[:, :, first : first + 256].reshape(n * cap, 256)
        total = jnp.dot(weigh[0], table, preferred_element_type=jnp.float32) + jnp.dot(
            weigh[1], table, preferred_element_type=jnp.float32
        )
        moe_out[:, first : first + 256] = total.astype(jnp.bfloat16)

    mix_part_copy.wait_recv()
    mix_sum_copy.wait_recv()
    mixer_out[...] = (
        shares[tp].astype(jnp.float32)
        + mix_part[...].astype(jnp.float32)
        + mix_in[...].astype(jnp.float32)
    ).astype(jnp.bfloat16)

    for made in (mix_part_copy, mix_pair_copy, mix_sum_copy):
        made.wait_send()
    for stage in range(1, floors):

        @pl.when((floor >= stage - 1) & (floor < floors - 1))
        def _():
            kv_z_copy(stage).wait_send()

    for stage in range(floors):

        @pl.when(floor >= stage)
        def _():
            kv_y_copy(stage).wait_send()

    for made in all_sent():
        made.wait_send()


def run_exchange(
    n, cap, tokens_in, moe_gain, routes, route_weights, queries_a, queries_b, head_gain,
    lambdas, keys_a, keys_b, values, w_gate, w_up, w_down, w_out,
):
    count, width = tokens_in.shape
    units = w_gate.shape[1]
    block = (n, cap, width)
    tokens = keys_a.shape[0]
    kv_width = keys_a.shape[1] + keys_b.shape[1] + values.shape[1]
    quarter = (tokens // 4, width)
    vmem = pl.BlockSpec(memory_space=pltpu.VMEM)
    hbm = pl.BlockSpec(memory_space=pltpu.HBM)
    call = pl.pallas_call(
        functools.partial(exchange, n),
        out_shape=(
            pltpu.VMEM((count, width), jnp.bfloat16),
            pltpu.VMEM(quarter, jnp.bfloat16),
        ),
        in_specs=[hbm] * 15,
        out_specs=(vmem, vmem),
        scratch_shapes=[
            pltpu.VMEM(tokens_in.shape, jnp.bfloat16),
            pltpu.VMEM((1, width), jnp.float32),
            pltpu.VMEM((TOP, count), jnp.int32),
            pltpu.VMEM((TOP, count), jnp.float32),
            pltpu.VMEM(queries_a.shape, jnp.bfloat16),
            pltpu.VMEM(queries_b.shape, jnp.bfloat16),
            pltpu.VMEM((1, VDIM), jnp.float32),
            pltpu.SMEM(lambdas.shape, jnp.float32),
            pltpu.VMEM(block, jnp.bfloat16),
            pltpu.VMEM(block, jnp.bfloat16),
            pltpu.VMEM((2, count, n * cap), jnp.bfloat16),
            pltpu.VMEM((n, 4, cap, width), jnp.bfloat16),
            pltpu.VMEM((n, 4, cap, width), jnp.bfloat16),
            pltpu.VMEM((2,) + block, jnp.bfloat16),
            pltpu.VMEM(block, jnp.bfloat16),
            pltpu.VMEM(block, jnp.bfloat16),
            pltpu.VMEM(block, jnp.bfloat16),
            pltpu.VMEM((4 * cap, units), jnp.bfloat16),
            pltpu.VMEM(w_gate.shape, jnp.bfloat16),
            pltpu.VMEM(w_up.shape, jnp.bfloat16),
            pltpu.VMEM(w_down.shape, jnp.bfloat16),
            pltpu.VMEM(w_out.shape, jnp.bfloat16),
            pltpu.VMEM((n, tokens, kv_width), jnp.bfloat16),
            pltpu.VMEM((tokens, w_out.shape[0]), jnp.bfloat16),
            pltpu.VMEM((4,) + quarter, jnp.bfloat16),
            pltpu.VMEM(quarter, jnp.bfloat16),
            pltpu.VMEM(quarter, jnp.bfloat16),
            pltpu.VMEM(quarter, jnp.bfloat16),
            pltpu.VMEM(quarter, jnp.bfloat16),
            pltpu.SemaphoreType.DMA((15,)),
            pltpu.SemaphoreType.DMA((5 * n + 13,)),
            pltpu.SemaphoreType.DMA((15,)),
        ],
        compiler_params=pltpu.CompilerParams(
            collective_id=0, has_side_effects=True, vmem_limit_bytes=48 * 2**20
        ),
        name="exchange",
    )
    operands = (
        tokens_in, moe_gain.reshape(1, -1), routes.T, route_weights.T,
        queries_a, queries_b, head_gain.reshape(1, -1), lambdas,
        keys_a, keys_b, values, w_gate, w_up, w_down, w_out,
    )
    return call(*[pltpu.with_memory_space_constraint(x, pltpu.HBM) for x in operands])


def fast_body(
    queries_a, queries_b, keys_a, keys_b, values, lambdas, head_gain, w_out,
    moe_tokens, moe_gain, routes, route_weights, w_gate, w_up, w_down,
):
    n = lax.axis_size("ep")
    cap = 3 * moe_tokens.shape[0] * TOP // (2 * n)
    moe_out, mixer_out = run_exchange(
        n, cap, moe_tokens, moe_gain, routes, route_weights, queries_a, queries_b,
        head_gain, lambdas, keys_a, keys_b, values, w_gate[0], w_up[0], w_down[0], w_out,
    )
    return (mixer_out, moe_out)


def whole_body(*args):
    n, n_tp = lax.axis_size("ep"), lax.axis_size("tp")
    tok_rows, w_gate = args[8].shape[0], args[12]
    cap = 3 * tok_rows * TOP // (2 * n)
    if w_gate.shape[0] == 1 and n_tp == 4 and n == 8 and cap % 16 == 0:
        return fast_body(*args)
    return body(*args)


def solution(mesh):
    return jax.shard_map(
        whole_body,
        mesh=mesh,
        in_specs=(
            P("ep", "tp"),
            P("ep", "tp"),
            P("ep", "tp"),
            P("ep", "tp"),
            P("ep", "tp"),
            P("tp"),
            P(),
            P("tp", None),
            P(("ep", "tp"), None),
            P(),
            P(("ep", "tp"), None),
            P(("ep", "tp"), None),
            P("ep", None, "tp"),
            P("ep", None, "tp"),
            P("ep", "tp", None),
        ),
        out_specs=(P(("ep", "tp"), None), P(("ep", "tp"), None)),
        check_vma=False,
    )
```

```python
import functools

import jax
import jax.numpy as jnp
from jax import lax
from jax.experimental import pallas as pl
from jax.experimental.pallas import tpu as pltpu
from jax.sharding import PartitionSpec as P

HEAD = 64
VDIM = 128
TOP = 2


eps = 1e-05
alpha_act = 1.702
limit_act = 7.0
negative = -1e30


def clamped_unit(gate, up):
    capped = jnp.minimum(gate, limit_act)
    linear = jnp.clip(up, -limit_act, limit_act)
    return capped * jax.nn.sigmoid(alpha_act * capped) * (linear + 1.0)


def hidden_rows(inputs, gate_matrix, up_matrix):
    gate = jnp.dot(inputs, gate_matrix, preferred_element_type=jnp.float32)
    up = jnp.dot(inputs, up_matrix, preferred_element_type=jnp.float32)
    return clamped_unit(gate, up).astype(jnp.bfloat16)


def pick_rows(table, owner):
    valid = owner < table.shape[0]
    chosen = jnp.take(table, jnp.minimum(owner, table.shape[0] - 1), axis=0)
    return jnp.where(valid[:, None], chosen, jnp.zeros_like(chosen))


def mixer(queries_a, queries_b, keys_a, keys_b, values, lambdas, head_gain, w_out):
    tokens = queries_a.shape[0]
    local_heads = lambdas.shape[0]
    kv_local = keys_a.shape[1] // HEAD
    group = local_heads // kv_local
    scale = HEAD ** (-0.5)
    query_pos = lax.axis_index("ep") * tokens + jnp.arange(tokens, dtype=jnp.int32)
    grouped_a = queries_a.reshape(tokens, kv_local, group, HEAD)
    grouped_b = queries_b.reshape(tokens, kv_local, group, HEAD)
    lowest = jnp.full((kv_local, group, tokens), negative, jnp.float32)
    nothing = jnp.zeros((kv_local, group, tokens), jnp.float32)
    blank = jnp.zeros((kv_local, group, tokens, VDIM), jnp.float32)

    def one_map(grouped, keys, value_rows, visible, state):
        peak, total, accum = state
        scores = (
            jnp.einsum("rgjd,ngd->gjrn", grouped, keys, preferred_element_type=jnp.float32) * scale
        )
        scores = jnp.where(visible, scores, negative)
        new_peak = jnp.maximum(peak, jnp.max(scores, axis=-1))
        expo = jnp.where(visible, jnp.exp(scores - new_peak[..., None]), 0.0)
        total = jnp.sum(expo, axis=-1)
        accum = jnp.einsum(
            "gjrn,ngv->gjrv",
            expo.astype(jnp.bfloat16),
            value_rows,
            preferred_element_type=jnp.float32,
        )
        return (new_peak, total, accum)

    initial = (lowest, nothing, blank, lowest, nothing, blank)
    piece_a = lax.all_gather(keys_a, "ep", axis=0, tiled=True)
    piece_b = lax.all_gather(keys_b, "ep", axis=0, tiled=True)
    piece_v = lax.all_gather(values, "ep", axis=0, tiled=True)
    count = piece_a.shape[0]

    def visit(state):
        key_pos = jnp.arange(count, dtype=jnp.int32)
        visible = key_pos[None, :] <= query_pos[:, None]
        value_rows = piece_v.reshape(count, kv_local, VDIM)
        first = one_map(
            grouped_a, piece_a.reshape(count, kv_local, HEAD), value_rows, visible, state[:3]
        )
        second = one_map(
            grouped_b, piece_b.reshape(count, kv_local, HEAD), value_rows, visible, state[3:]
        )
        return first + second

    result = lax.cond(jnp.int32(0) <= query_pos[tokens - 1], visit, lambda state: state, initial)
    mixed_a = result[2] / result[1][..., None]
    mixed_b = result[5] / result[4][..., None]
    diff = mixed_a - lambdas.reshape(kv_local, group, 1, 1) * mixed_b
    heads_out = (
        diff * lax.rsqrt(jnp.mean(diff * diff, axis=-1, keepdims=True) + eps) * head_gain
    ).astype(jnp.bfloat16)
    weights_out = w_out.reshape(kv_local, group, VDIM, w_out.shape[1])
    return lax.psum_scatter(
        jnp.einsum(
            "gjrv,gjvd->rd", heads_out, weights_out, preferred_element_type=jnp.float32
        ).astype(jnp.bfloat16),
        "tp",
        scatter_dimension=0,
        tiled=True,
    )


def experts(moe_tokens, moe_gain, routes, route_weights, w_gate, w_up, w_down):
    tok_rows, width = moe_tokens.shape
    n_experts = lax.axis_size("ep") * w_gate.shape[0]
    capacity = max(2, 3 * tok_rows * TOP // (2 * n_experts))
    inputs = moe_tokens.astype(jnp.float32)
    normed = (
        inputs * lax.rsqrt(jnp.mean(inputs * inputs, axis=-1, keepdims=True) + eps) * moe_gain
    ).astype(jnp.bfloat16)
    chosen = routes.reshape(-1)
    member = (chosen[:, None] == jnp.arange(n_experts, dtype=jnp.int32)[None, :]).astype(jnp.int32)
    order_in = jnp.sum(jnp.cumsum(member, axis=0) * member, axis=1) - 1
    slot_ids = chosen * capacity + order_in
    owner = (
        jnp.full((n_experts * capacity,), tok_rows, jnp.int32)
        .at[slot_ids]
        .set(jnp.arange(tok_rows * TOP, dtype=jnp.int32) // TOP)
    )
    outgoing = pick_rows(normed, owner).reshape(n_experts, capacity, width)
    arrived = lax.all_to_all(outgoing, "ep", split_axis=0, concat_axis=1, tiled=True).reshape(
        -1, width
    )
    hidden = hidden_rows(lax.all_gather(arrived, "tp", axis=0, tiled=True), w_gate[0], w_up[0])
    expert_out = lax.psum_scatter(
        jnp.dot(hidden, w_down[0], preferred_element_type=jnp.float32).astype(jnp.bfloat16),
        "tp",
        scatter_dimension=0,
        tiled=True,
    )
    returned = lax.all_to_all(
        expert_out.reshape(-1, capacity, width), "ep", split_axis=0, concat_axis=0, tiled=True
    )
    picked = jnp.take(returned.reshape(-1, width), slot_ids, axis=0).reshape(tok_rows, TOP, width)
    return jnp.sum(picked.astype(jnp.float32) * route_weights[:, :, None], axis=1).astype(
        jnp.bfloat16
    )


def body(
    queries_a,
    queries_b,
    keys_a,
    keys_b,
    values,
    lambdas,
    head_gain,
    w_out,
    moe_tokens,
    moe_gain,
    routes,
    route_weights,
    w_gate,
    w_up,
    w_down,
):
    mixer_out = mixer(queries_a, queries_b, keys_a, keys_b, values, lambdas, head_gain, w_out)
    moe_out = experts(moe_tokens, moe_gain, routes, route_weights, w_gate, w_up, w_down)
    return (mixer_out, moe_out)


MESH = pl.DeviceIdType.MESH
OUT, ACROSS, CORE, PAIR, PART, KV_Z, KV_Y, MIX, BACK, RELAYS, HALVES, TRIPS = range(12)


def xor(first, second, limit):
    total, bit = 0, 1
    while bit < limit:
        total = total + (first // bit + second // bit) % 2 * bit
        bit *= 2
    return total


def exchange(
    n, moe_tokens, gain_in, routes_in, weights_in, queries_a_in, queries_b_in, head_gain_in, lambdas_in,
    keys_a, keys_b, values, w_gate, w_up, w_down, w_out,
    moe_out, mixer_out,
    tokens_in, moe_gain, routes, route_weights, queries_a, queries_b, head_gain, lambdas,
    ret, outgoing, weigh, rows, parts, part_in, pair_in, sums, final, hidden, gate_v, up_v, down_v, out_v,
    kv_all, heads, shares, mix_part, mix_pair, mix_in, mix_sum, send, recv, local,
):
    me = lax.axis_index("ep")
    tp = lax.axis_index("tp")
    core = tp + 1 - 2 * (tp % 2)
    across = tp + 2 - 4 * (tp // 2)
    diagonal = core + 2 - 4 * (core // 2)
    floor, lane = me // 2, me % 2
    floors = n // 2
    cap, width = outgoing.shape[1:]
    units = hidden.shape[1]
    flat = 4 * cap
    tokens = kv_all.shape[1]

    inner = (floor + 1) // 2 % 2

    def order(step):
        turn = step // 2
        return step + inner * (2 * (turn // 2 + 2 * (turn % 2)) + step % 2 - step)

    def partner(k):
        return xor(me, k, n)

    def place_of(kind, k):
        return n * kind + k if kind < KV_Z else 5 * n + 4 * (kind - KV_Z) + k

    def sent_by(kind, k):
        return kind - BACK if kind > BACK else 3 + 4 * (kind - KV_Z) + k

    def copy(kind, k, group, source, target, device):
        return pltpu.make_async_remote_copy(
            src_ref=source,
            dst_ref=target,
            send_sem=send.at[sent_by(group, k)],
            recv_sem=recv.at[place_of(kind, k)],
            device_id=device,
            device_id_type=MESH,
        )

    def out_copy(k):
        return copy(OUT, k, TRIPS, outgoing.at[partner(k)], rows.at[k, 0], {"ep": partner(k)})

    def core_copy(k):
        return copy(CORE, k, RELAYS, rows.at[k, 0], rows.at[k, 1], {"tp": core})

    def across_copy(k):
        return copy(ACROSS, k, RELAYS, rows.at[k, 0], rows.at[k, 2], {"tp": across})

    def core_across_copy(k):
        return copy(CORE, k, RELAYS, rows.at[k, 2], rows.at[k, 3], {"tp": core})

    def both_core_copies(k):
        return copy(CORE, k, RELAYS, rows.at[k, 0:2], rows.at[k, 2:4], {"tp": core})

    def part_copy(k):
        return copy(PART, k, HALVES, parts.at[k, 1], part_in.at[0, k], {"tp": core})

    def pair_copy(k):
        return copy(PAIR, k, HALVES, parts.at[k, 3], pair_in.at[k], {"tp": core})

    def sums_copy(k):
        return copy(PART, k, RELAYS, sums.at[k], part_in.at[1, k], {"tp": across})

    def part_and_sums(k):
        return copy(PART, k, RELAYS, rows.at[k, 0:2], part_in.at[:, k], {"tp": across})

    def back_copy(k):
        return copy(BACK, 0, TRIPS, final.at[k], ret.at[me], {"ep": partner(k)})

    def all_back():
        return copy(BACK, 0, TRIPS, final.at[0 : n - 1], ret.at[0 : n - 1], {"tp": core})

    def all_sent():
        return [
            copy(OUT, 0, RELAYS, rows, rows, {"tp": core}),
            copy(OUT, 0, HALVES, rows.at[:, 0:2], rows.at[:, 0:2], {"tp": core}),
            copy(OUT, 0, TRIPS, rows.at[0 : n - 1, 0:2], rows.at[0 : n - 1, 0:2], {"tp": core}),
        ]

    def kv_z_copy(stage):
        block = kv_all.at[2 * (floor - stage + 1) + lane]
        return copy(KV_Z, stage, KV_Z, block, block, {"ep": me + 2})

    def kv_y_copy(stage):
        block = kv_all.at[2 * (floor - stage) + lane]
        return copy(KV_Y, stage, KV_Y, block, block, {"ep": me + 1 - 2 * lane})

    mix_part_copy = copy(MIX, 0, MIX, shares.at[core], mix_part, {"tp": core})
    mix_pair_copy = copy(MIX, 1, MIX, shares.at[diagonal], mix_pair, {"tp": core})
    mix_sum_copy = copy(MIX, 2, MIX, mix_sum, mix_in, {"tp": across})

    local_heads = heads.shape[1] // VDIM
    kv_local = kv_all.shape[2] // (2 * HEAD + VDIM)
    span = kv_local * HEAD

    def one_map(queries, head, offset):
        g = head // (local_heads // kv_local)
        count = n * tokens
        first = offset + g * HEAD
        keys = kv_all[:, :, first : first + HEAD].reshape(count, HEAD)
        first = 2 * span + g * VDIM
        value_rows = kv_all[:, :, first : first + VDIM].reshape(count, VDIM)
        scores = lax.dot_general(
            queries[:, head * HEAD : (head + 1) * HEAD],
            keys,
            (((1,), (1,)), ((), ())),
            preferred_element_type=jnp.float32,
        ) * HEAD ** (-0.5)
        query_pos = me * tokens + lax.broadcasted_iota(jnp.int32, scores.shape, 0)
        key_pos = lax.broadcasted_iota(jnp.int32, scores.shape, 1)
        scores = jnp.where(key_pos <= query_pos, scores, negative)
        expo = jnp.exp(scores - jnp.max(scores, axis=1, keepdims=True))
        total = jnp.sum(expo, axis=1, keepdims=True)
        mixed = jnp.dot(
            expo.astype(jnp.bfloat16), value_rows, preferred_element_type=jnp.float32
        )
        return mixed / total

    def attend(head):
        diff = one_map(queries_a, head, 0) - lambdas[head] * one_map(queries_b, head, span)
        norm = lax.rsqrt(jnp.mean(diff * diff, axis=1, keepdims=True) + eps)
        heads[:, head * VDIM : (head + 1) * VDIM] = (diff * norm * head_gain[...]).astype(
            jnp.bfloat16
        )

    def forward(k):
        core_copy(k).start()
        across_copy(k).start()

    def relay(k):
        across_copy(k).wait_recv()
        core_across_copy(k).start()

    def send_sums(k):
        pair_copy(k).wait_recv()
        sums[k] = (
            parts[k, 2].astype(jnp.float32) + pair_in[k].astype(jnp.float32)
        ).astype(jnp.bfloat16)
        sums_copy(k).start()

    def finish(k):
        part_and_sums(k).wait_recv()
        return (
            parts[k, 0].astype(jnp.float32)
            + part_in[0, k].astype(jnp.float32)
            + part_in[1, k].astype(jnp.float32)
        ).astype(jnp.bfloat16)

    def send_back(k):
        final[k] = finish(k)
        back_copy(k).start()

    def feed(k):
        both_core_copies(k).wait_recv()
        inputs = rows[k].reshape(flat, width)
        step = min(256, units)
        for first in range(0, units, step):
            gate = jnp.dot(
                inputs, gate_v[:, first : first + step], preferred_element_type=jnp.float32
            )
            up = jnp.dot(
                inputs, up_v[:, first : first + step], preferred_element_type=jnp.float32
            )
            hidden[:, first : first + step] = clamped_unit(gate, up).astype(jnp.bfloat16)
        for first in range(0, width, 256):
            piece = jnp.dot(
                hidden[...], down_v[:, first : first + 256], preferred_element_type=jnp.float32
            )
            parts[k, :, :, first : first + 256] = piece.astype(jnp.bfloat16).reshape(
                4, cap, 256
            )
        pair_copy(k).start()
        part_copy(k).start()

    barrier = pltpu.get_barrier_semaphore()
    for shift in range(1, n):
        pl.semaphore_signal(
            barrier, inc=1, device_id={"ep": (me + shift) % n}, device_id_type=MESH
        )
    for shift in range(1, 4):
        pl.semaphore_signal(
            barrier, inc=1, device_id={"tp": (tp + shift) % 4}, device_id_type=MESH
        )

    pairs = [
        (moe_tokens, tokens_in), (gain_in, moe_gain), (routes_in, routes),
        (keys_a, kv_all.at[me, :, 0:span]), (keys_b, kv_all.at[me, :, span : 2 * span]),
        (values, kv_all.at[me, :, 2 * span :]), (weights_in, route_weights),
        (w_gate, gate_v), (w_up, up_v), (w_down, down_v), (w_out, out_v),
        (queries_a_in, queries_a), (queries_b_in, queries_b), (head_gain_in, head_gain),
        (lambdas_in, lambdas),
    ]
    loads = [
        pltpu.make_async_copy(source, target, local.at[i])
        for i, (source, target) in enumerate(pairs)
    ]
    for load in loads:
        load.start()
    for load in loads[:3]:
        load.wait()

    inputs = tokens_in[...].astype(jnp.float32)
    normed = (
        inputs
        * lax.rsqrt(jnp.mean(inputs * inputs, axis=1, keepdims=True) + eps)
        * moe_gain[...]
    ).astype(jnp.bfloat16)
    count = tokens_in.shape[0]
    expert = lax.broadcasted_iota(jnp.int32, (n, count), 0)
    named = [routes[k : k + 1, :] == expert for k in range(TOP)]
    member = named[0]
    for k in range(1, TOP):
        member = member | named[k]
    earlier = lax.broadcasted_iota(jnp.int32, (count, count), 0) < lax.broadcasted_iota(
        jnp.int32, (count, count), 1
    )
    place = jnp.dot(
        jnp.where(member, 1.0, 0.0).astype(jnp.bfloat16),
        jnp.where(earlier, 1.0, 0.0).astype(jnp.bfloat16),
        preferred_element_type=jnp.float32,
    )
    position = lax.broadcasted_iota(jnp.int32, (cap, count), 0).astype(jnp.float32)
    slot = jnp.where(member, place, -1.0)
    for e in range(n):
        pick = jnp.where(slot[e : e + 1, :] == position, 1.0, 0.0).astype(jnp.bfloat16)
        outgoing[e] = jnp.dot(pick, normed, preferred_element_type=jnp.float32).astype(
            jnp.bfloat16
        )
    rows[0, 0] = outgoing[me]
    pl.semaphore_wait(barrier, n + 2)

    forward(0)
    for k in (1, 4):
        out_copy(k).start()
    out_copy(5 - 3 * inner).start()

    for other in range(1, floors):

        @pl.when(floor < other)
        def _():
            for side in range(2):
                kv_all[2 * other + side] = jnp.zeros(kv_all.shape[1:], jnp.bfloat16)

    for load in loads[3:7]:
        load.wait()
    share = route_weights[...]
    scale = jnp.where(named[0], share[0:1, :], 0.0)
    for k in range(1, TOP):
        scale = scale + jnp.where(named[k], share[k : k + 1, :], 0.0)
    table = jnp.concatenate(
        [
            jnp.where(slot[e : e + 1, :] == position, scale[e : e + 1, :], 0.0)
            for e in range(n)
        ],
        axis=0,
    ).T
    high = table.astype(jnp.bfloat16)
    weigh[0:count] = high
    weigh[count:] = (table - high.astype(jnp.float32)).astype(jnp.bfloat16)
    out_copy(2 + 3 * inner).start()
    for load in loads[7:]:
        load.wait()

    def kv_next(stage):
        @pl.when(floor >= stage)
        def _():
            kv_z_copy(stage).wait_recv()
            kv_y_copy(stage).start()
            if stage < floors - 1:

                @pl.when(floor < floors - 1)
                def _():
                    kv_z_copy(stage + 1).start()

    def pass_on(k):
        out_copy(k).wait_recv()
        forward(k)

    @pl.loop(0, n)
    def _(step):
        @pl.when(step == 3)
        def _():
            send_sums(1)

        @pl.when(step < 5)
        def _():
            pass_on(order(step + 1))

        for k in (6, 7):

            @pl.when(step == k - 2 + inner)
            def _():
                pass_on(k)

        for k in (4, 5):

            @pl.when(step == k + 2 - inner)
            def _():
                send_sums(k)

        @pl.when(step == 0)
        def _():
            out_copy(3).start()
            out_copy(6).start()

        @pl.when(step == 1)
        def _():
            out_copy(7).start()

        @pl.when(step == 2)
        def _():
            @pl.when(floor < floors - 1)
            def _():
                kv_z_copy(1).start()

            kv_y_copy(0).start()

        @pl.when(step == 5)
        def _():
            send_back(1)

        @pl.when(step == 6)
        def _():
            kv_next(1)

        @pl.when((step == 7) & (inner == 1))
        def _():
            send_sums(6)
            send_back(4)

        @pl.when(step == 7)
        def _():
            kv_next(2)

        relay(order(step))
        feed(order(step))

    @pl.when(inner == 0)
    def _():
        send_sums(6)

    send_sums(7)

    @pl.when(inner == 0)
    def _():
        send_back(4)

    send_back(5)
    send_sums(3)
    send_sums(2)
    kv_next(3)
    for stage in range(floors):

        @pl.when(floor >= stage)
        def _():
            kv_y_copy(stage).wait_recv()

    for head in range(local_heads):
        attend(head)
    send_back(6)
    for first in range(0, width, 256):
        piece = jnp.dot(
            heads[...], out_v[:, first : first + 256], preferred_element_type=jnp.float32
        )
        shares[:, :, first : first + 256] = piece.astype(jnp.bfloat16).reshape(
            4, tokens // 4, 256
        )
    mix_pair_copy.start()
    mix_part_copy.start()
    send_back(7)
    mix_pair_copy.wait_recv()
    mix_sum[...] = (
        shares[across].astype(jnp.float32) + mix_pair[...].astype(jnp.float32)
    ).astype(jnp.bfloat16)
    mix_sum_copy.start()
    send_sums(0)
    send_back(3)
    send_back(2)
    ret[me] = finish(0)

    all_back().wait_recv()
    for first in range(0, width, 256):
        table = ret[:, :, first : first + 256].reshape(n * cap, 256)
        total = jnp.dot(weigh[...], table, preferred_element_type=jnp.float32)
        moe_out[:, first : first + 256] = (total[:count] + total[count:]).astype(jnp.bfloat16)

    mix_part_copy.wait_recv()
    mix_sum_copy.wait_recv()
    mixer_out[...] = (
        shares[tp].astype(jnp.float32)
        + mix_part[...].astype(jnp.float32)
        + mix_in[...].astype(jnp.float32)
    ).astype(jnp.bfloat16)

    for made in (mix_part_copy, mix_pair_copy, mix_sum_copy):
        made.wait_send()
    for stage in range(1, floors):

        @pl.when((floor >= stage - 1) & (floor < floors - 1))
        def _():
            kv_z_copy(stage).wait_send()

    for stage in range(floors):

        @pl.when(floor >= stage)
        def _():
            kv_y_copy(stage).wait_send()

    for made in all_sent():
        made.wait_send()


def settle(first, second, first_out, second_out, sems):
    copies = [
        pltpu.make_async_copy(first, first_out, sems.at[0]),
        pltpu.make_async_copy(second, second_out, sems.at[1]),
    ]
    for made in copies:
        made.start()
    for made in copies:
        made.wait()


def run_exchange(
    n, cap, tokens_in, moe_gain, routes, route_weights, queries_a, queries_b, head_gain,
    lambdas, keys_a, keys_b, values, w_gate, w_up, w_down, w_out,
):
    count, width = tokens_in.shape
    units = w_gate.shape[1]
    block = (n, cap, width)
    tokens = keys_a.shape[0]
    kv_width = keys_a.shape[1] + keys_b.shape[1] + values.shape[1]
    quarter = (tokens // 4, width)
    vmem = pl.BlockSpec(memory_space=pltpu.VMEM)
    hbm = pl.BlockSpec(memory_space=pltpu.HBM)
    call = pl.pallas_call(
        functools.partial(exchange, n),
        out_shape=(
            pltpu.VMEM((count, width), jnp.bfloat16),
            pltpu.VMEM(quarter, jnp.bfloat16),
        ),
        in_specs=[hbm] * 15,
        out_specs=(vmem, vmem),
        scratch_shapes=[
            pltpu.VMEM(tokens_in.shape, jnp.bfloat16),
            pltpu.VMEM((1, width), jnp.float32),
            pltpu.VMEM((TOP, count), jnp.int32),
            pltpu.VMEM((TOP, count), jnp.float32),
            pltpu.VMEM(queries_a.shape, jnp.bfloat16),
            pltpu.VMEM(queries_b.shape, jnp.bfloat16),
            pltpu.VMEM((1, VDIM), jnp.float32),
            pltpu.SMEM(lambdas.shape, jnp.float32),
            pltpu.VMEM(block, jnp.bfloat16),
            pltpu.VMEM(block, jnp.bfloat16),
            pltpu.VMEM((2 * count, n * cap), jnp.bfloat16),
            pltpu.VMEM((n, 4, cap, width), jnp.bfloat16),
            pltpu.VMEM((n, 4, cap, width), jnp.bfloat16),
            pltpu.VMEM((2,) + block, jnp.bfloat16),
            pltpu.VMEM(block, jnp.bfloat16),
            pltpu.VMEM(block, jnp.bfloat16),
            pltpu.VMEM(block, jnp.bfloat16),
            pltpu.VMEM((4 * cap, units), jnp.bfloat16),
            pltpu.VMEM(w_gate.shape, jnp.bfloat16),
            pltpu.VMEM(w_up.shape, jnp.bfloat16),
            pltpu.VMEM(w_down.shape, jnp.bfloat16),
            pltpu.VMEM(w_out.shape, jnp.bfloat16),
            pltpu.VMEM((n, tokens, kv_width), jnp.bfloat16),
            pltpu.VMEM((tokens, w_out.shape[0]), jnp.bfloat16),
            pltpu.VMEM((4,) + quarter, jnp.bfloat16),
            pltpu.VMEM(quarter, jnp.bfloat16),
            pltpu.VMEM(quarter, jnp.bfloat16),
            pltpu.VMEM(quarter, jnp.bfloat16),
            pltpu.VMEM(quarter, jnp.bfloat16),
            pltpu.SemaphoreType.DMA((15,)),
            pltpu.SemaphoreType.DMA((5 * n + 13,)),
            pltpu.SemaphoreType.DMA((15,)),
        ],
        compiler_params=pltpu.CompilerParams(
            collective_id=0, has_side_effects=True, vmem_limit_bytes=48 * 2**20
        ),
        name="exchange",
    )
    operands = (
        tokens_in, moe_gain.reshape(1, -1), routes.T, route_weights.T,
        queries_a, queries_b, head_gain.reshape(1, -1), lambdas,
        keys_a, keys_b, values, w_gate, w_up, w_down, w_out,
    )
    made = call(*[pltpu.with_memory_space_constraint(x, pltpu.HBM) for x in operands])
    return pl.pallas_call(
        settle,
        out_shape=tuple(jax.ShapeDtypeStruct(x.shape, x.dtype) for x in made),
        in_specs=[vmem] * 2,
        out_specs=(hbm, hbm),
        scratch_shapes=[pltpu.SemaphoreType.DMA((2,))],
        compiler_params=pltpu.CompilerParams(vmem_limit_bytes=2**20),
        name="settle",
    )(*[pltpu.with_memory_space_constraint(x, pltpu.VMEM) for x in made])


def fast_body(
    queries_a, queries_b, keys_a, keys_b, values, lambdas, head_gain, w_out,
    moe_tokens, moe_gain, routes, route_weights, w_gate, w_up, w_down,
):
    n = lax.axis_size("ep")
    cap = 3 * moe_tokens.shape[0] * TOP // (2 * n)
    moe_out, mixer_out = run_exchange(
        n, cap, moe_tokens, moe_gain, routes, route_weights, queries_a, queries_b,
        head_gain, lambdas, keys_a, keys_b, values, w_gate[0], w_up[0], w_down[0], w_out,
    )
    return (mixer_out, moe_out)


def whole_body(*args):
    n, n_tp = lax.axis_size("ep"), lax.axis_size("tp")
    tok_rows, w_gate = args[8].shape[0], args[12]
    cap = 3 * tok_rows * TOP // (2 * n)
    if w_gate.shape[0] == 1 and n_tp == 4 and n == 8 and cap % 16 == 0:
        return fast_body(*args)
    return body(*args)


def solution(mesh):
    return jax.shard_map(
        whole_body,
        mesh=mesh,
        in_specs=(
            P("ep", "tp"),
            P("ep", "tp"),
            P("ep", "tp"),
            P("ep", "tp"),
            P("ep", "tp"),
            P("tp"),
            P(),
            P("tp", None),
            P(("ep", "tp"), None),
            P(),
            P(("ep", "tp"), None),
            P(("ep", "tp"), None),
            P("ep", None, "tp"),
            P("ep", None, "tp"),
            P("ep", "tp", None),
        ),
        out_specs=(P(("ep", "tp"), None), P(("ep", "tp"), None)),
        check_vma=False,
    )
```

```python
import functools

import jax
import jax.numpy as jnp
from jax import lax
from jax.experimental import pallas as pl
from jax.experimental.pallas import tpu as pltpu
from jax.sharding import PartitionSpec as P

HEAD = 64
VDIM = 128
TOP = 2


eps = 1e-05
alpha_act = 1.702
limit_act = 7.0
negative = -1e30


def clamped_unit(gate, up):
    capped = jnp.minimum(gate, limit_act)
    linear = jnp.clip(up, -limit_act, limit_act)
    return capped * jax.nn.sigmoid(alpha_act * capped) * (linear + 1.0)


def hidden_rows(inputs, gate_matrix, up_matrix):
    gate = jnp.dot(inputs, gate_matrix, preferred_element_type=jnp.float32)
    up = jnp.dot(inputs, up_matrix, preferred_element_type=jnp.float32)
    return clamped_unit(gate, up).astype(jnp.bfloat16)


def pick_rows(table, owner):
    valid = owner < table.shape[0]
    chosen = jnp.take(table, jnp.minimum(owner, table.shape[0] - 1), axis=0)
    return jnp.where(valid[:, None], chosen, jnp.zeros_like(chosen))


def mixer(queries_a, queries_b, keys_a, keys_b, values, lambdas, head_gain, w_out):
    tokens = queries_a.shape[0]
    local_heads = lambdas.shape[0]
    kv_local = keys_a.shape[1] // HEAD
    group = local_heads // kv_local
    scale = HEAD ** (-0.5)
    query_pos = lax.axis_index("ep") * tokens + jnp.arange(tokens, dtype=jnp.int32)
    grouped_a = queries_a.reshape(tokens, kv_local, group, HEAD)
    grouped_b = queries_b.reshape(tokens, kv_local, group, HEAD)
    lowest = jnp.full((kv_local, group, tokens), negative, jnp.float32)
    nothing = jnp.zeros((kv_local, group, tokens), jnp.float32)
    blank = jnp.zeros((kv_local, group, tokens, VDIM), jnp.float32)

    def one_map(grouped, keys, value_rows, visible, state):
        peak, total, accum = state
        scores = (
            jnp.einsum("rgjd,ngd->gjrn", grouped, keys, preferred_element_type=jnp.float32) * scale
        )
        scores = jnp.where(visible, scores, negative)
        new_peak = jnp.maximum(peak, jnp.max(scores, axis=-1))
        expo = jnp.where(visible, jnp.exp(scores - new_peak[..., None]), 0.0)
        total = jnp.sum(expo, axis=-1)
        accum = jnp.einsum(
            "gjrn,ngv->gjrv",
            expo.astype(jnp.bfloat16),
            value_rows,
            preferred_element_type=jnp.float32,
        )
        return (new_peak, total, accum)

    initial = (lowest, nothing, blank, lowest, nothing, blank)
    piece_a = lax.all_gather(keys_a, "ep", axis=0, tiled=True)
    piece_b = lax.all_gather(keys_b, "ep", axis=0, tiled=True)
    piece_v = lax.all_gather(values, "ep", axis=0, tiled=True)
    count = piece_a.shape[0]

    def visit(state):
        key_pos = jnp.arange(count, dtype=jnp.int32)
        visible = key_pos[None, :] <= query_pos[:, None]
        value_rows = piece_v.reshape(count, kv_local, VDIM)
        first = one_map(
            grouped_a, piece_a.reshape(count, kv_local, HEAD), value_rows, visible, state[:3]
        )
        second = one_map(
            grouped_b, piece_b.reshape(count, kv_local, HEAD), value_rows, visible, state[3:]
        )
        return first + second

    result = lax.cond(jnp.int32(0) <= query_pos[tokens - 1], visit, lambda state: state, initial)
    mixed_a = result[2] / result[1][..., None]
    mixed_b = result[5] / result[4][..., None]
    diff = mixed_a - lambdas.reshape(kv_local, group, 1, 1) * mixed_b
    heads_out = (
        diff * lax.rsqrt(jnp.mean(diff * diff, axis=-1, keepdims=True) + eps) * head_gain
    ).astype(jnp.bfloat16)
    weights_out = w_out.reshape(kv_local, group, VDIM, w_out.shape[1])
    return lax.psum_scatter(
        jnp.einsum(
            "gjrv,gjvd->rd", heads_out, weights_out, preferred_element_type=jnp.float32
        ).astype(jnp.bfloat16),
        "tp",
        scatter_dimension=0,
        tiled=True,
    )


def experts(moe_tokens, moe_gain, routes, route_weights, w_gate, w_up, w_down):
    tok_rows, width = moe_tokens.shape
    n_experts = lax.axis_size("ep") * w_gate.shape[0]
    capacity = max(2, 3 * tok_rows * TOP // (2 * n_experts))
    inputs = moe_tokens.astype(jnp.float32)
    normed = (
        inputs * lax.rsqrt(jnp.mean(inputs * inputs, axis=-1, keepdims=True) + eps) * moe_gain
    ).astype(jnp.bfloat16)
    chosen = routes.reshape(-1)
    member = (chosen[:, None] == jnp.arange(n_experts, dtype=jnp.int32)[None, :]).astype(jnp.int32)
    order_in = jnp.sum(jnp.cumsum(member, axis=0) * member, axis=1) - 1
    slot_ids = chosen * capacity + order_in
    owner = (
        jnp.full((n_experts * capacity,), tok_rows, jnp.int32)
        .at[slot_ids]
        .set(jnp.arange(tok_rows * TOP, dtype=jnp.int32) // TOP)
    )
    outgoing = pick_rows(normed, owner).reshape(n_experts, capacity, width)
    arrived = lax.all_to_all(outgoing, "ep", split_axis=0, concat_axis=1, tiled=True).reshape(
        -1, width
    )
    hidden = hidden_rows(lax.all_gather(arrived, "tp", axis=0, tiled=True), w_gate[0], w_up[0])
    expert_out = lax.psum_scatter(
        jnp.dot(hidden, w_down[0], preferred_element_type=jnp.float32).astype(jnp.bfloat16),
        "tp",
        scatter_dimension=0,
        tiled=True,
    )
    returned = lax.all_to_all(
        expert_out.reshape(-1, capacity, width), "ep", split_axis=0, concat_axis=0, tiled=True
    )
    picked = jnp.take(returned.reshape(-1, width), slot_ids, axis=0).reshape(tok_rows, TOP, width)
    return jnp.sum(picked.astype(jnp.float32) * route_weights[:, :, None], axis=1).astype(
        jnp.bfloat16
    )


def body(
    queries_a,
    queries_b,
    keys_a,
    keys_b,
    values,
    lambdas,
    head_gain,
    w_out,
    moe_tokens,
    moe_gain,
    routes,
    route_weights,
    w_gate,
    w_up,
    w_down,
):
    mixer_out = mixer(queries_a, queries_b, keys_a, keys_b, values, lambdas, head_gain, w_out)
    moe_out = experts(moe_tokens, moe_gain, routes, route_weights, w_gate, w_up, w_down)
    return (mixer_out, moe_out)


MESH = pl.DeviceIdType.MESH
OUT, ACROSS, CORE, PAIR, PART, KV_Z, KV_Y, MIX, BACK, RELAYS, HALVES, TRIPS = range(12)


def xor(first, second, limit):
    total, bit = 0, 1
    while bit < limit:
        total = total + (first // bit + second // bit) % 2 * bit
        bit *= 2
    return total


def exchange(
    n, moe_tokens, gain_in, routes_in, weights_in, queries_a_in, queries_b_in, head_gain_in, lambdas_in,
    keys_a, keys_b, values, w_gate, w_up, w_down, w_out,
    moe_out, mixer_out,
    tokens_in, moe_gain, routes, route_weights, queries_a, queries_b, head_gain, lambdas,
    ret, outgoing, weigh, rows, parts, part_in, pair_in, sums, final, hidden, gate_v, up_v, down_v, out_v,
    kv_all, heads, shares, mix_part, mix_pair, mix_in, mix_sum, send, recv, local,
):
    me = lax.axis_index("ep")
    tp = lax.axis_index("tp")
    core = tp + 1 - 2 * (tp % 2)
    across = tp + 2 - 4 * (tp // 2)
    diagonal = core + 2 - 4 * (core // 2)
    floor, lane = me // 2, me % 2
    floors = n // 2
    cap, width = outgoing.shape[1:]
    units = hidden.shape[1]
    flat = 4 * cap
    tokens = kv_all.shape[1]

    inner = (floor + 1) // 2 % 2

    def order(step):
        turn = step // 2
        return step + inner * (2 * (turn // 2 + 2 * (turn % 2)) + step % 2 - step)

    def partner(k):
        return xor(me, k, n)

    def place_of(kind, k):
        return n * kind + k if kind < KV_Z else 5 * n + 4 * (kind - KV_Z) + k

    def sent_by(kind, k):
        return kind - BACK if kind > BACK else 3 + 4 * (kind - KV_Z) + k

    def copy(kind, k, group, source, target, device):
        return pltpu.make_async_remote_copy(
            src_ref=source,
            dst_ref=target,
            send_sem=send.at[sent_by(group, k)],
            recv_sem=recv.at[place_of(kind, k)],
            device_id=device,
            device_id_type=MESH,
        )

    def out_copy(k):
        return copy(OUT, k, TRIPS, outgoing.at[partner(k)], rows.at[k, 0], {"ep": partner(k)})

    def core_copy(k):
        return copy(CORE, k, RELAYS, rows.at[k, 0], rows.at[k, 1], {"tp": core})

    def across_copy(k):
        return copy(ACROSS, k, RELAYS, rows.at[k, 0], rows.at[k, 2], {"tp": across})

    def core_across_copy(k):
        return copy(CORE, k, RELAYS, rows.at[k, 2], rows.at[k, 3], {"tp": core})

    def both_core_copies(k):
        return copy(CORE, k, RELAYS, rows.at[k, 0:2], rows.at[k, 2:4], {"tp": core})

    def part_copy(k):
        return copy(PART, k, HALVES, parts.at[k, 1], part_in.at[0, k], {"tp": core})

    def pair_copy(k):
        return copy(PAIR, k, HALVES, parts.at[k, 3], pair_in.at[k], {"tp": core})

    def sums_copy(k):
        return copy(PART, k, RELAYS, sums.at[k], part_in.at[1, k], {"tp": across})

    def part_and_sums(k):
        return copy(PART, k, RELAYS, rows.at[k, 0:2], part_in.at[:, k], {"tp": across})

    def back_copy(k):
        return copy(BACK, 0, TRIPS, final.at[k], ret.at[me], {"ep": partner(k)})

    def all_back():
        return copy(BACK, 0, TRIPS, final.at[0 : n - 1], ret.at[0 : n - 1], {"tp": core})

    def all_sent():
        return [
            copy(OUT, 0, RELAYS, rows, rows, {"tp": core}),
            copy(OUT, 0, HALVES, rows.at[:, 0:2], rows.at[:, 0:2], {"tp": core}),
            copy(OUT, 0, TRIPS, rows.at[0 : n - 1, 0:2], rows.at[0 : n - 1, 0:2], {"tp": core}),
        ]

    def kv_z_copy(stage):
        block = kv_all.at[2 * (floor - stage + 1) + lane]
        return copy(KV_Z, stage, KV_Z, block, block, {"ep": me + 2})

    def kv_y_copy(stage):
        block = kv_all.at[2 * (floor - stage) + lane]
        return copy(KV_Y, stage, KV_Y, block, block, {"ep": me + 1 - 2 * lane})

    mix_part_copy = copy(MIX, 0, MIX, shares.at[core], mix_part, {"tp": core})
    mix_pair_copy = copy(MIX, 1, MIX, shares.at[diagonal], mix_pair, {"tp": core})
    mix_sum_copy = copy(MIX, 2, MIX, mix_sum, mix_in, {"tp": across})

    local_heads = heads.shape[1] // VDIM
    kv_local = kv_all.shape[2] // (2 * HEAD + VDIM)
    span = kv_local * HEAD

    def one_map(queries, head, offset):
        g = head // (local_heads // kv_local)
        count = n * tokens
        first = offset + g * HEAD
        keys = kv_all[:, :, first : first + HEAD].reshape(count, HEAD)
        first = 2 * span + g * VDIM
        value_rows = kv_all[:, :, first : first + VDIM].reshape(count, VDIM)
        scores = lax.dot_general(
            queries[:, head * HEAD : (head + 1) * HEAD],
            keys,
            (((1,), (1,)), ((), ())),
            preferred_element_type=jnp.float32,
        ) * HEAD ** (-0.5)
        query_pos = me * tokens + lax.broadcasted_iota(jnp.int32, scores.shape, 0)
        key_pos = lax.broadcasted_iota(jnp.int32, scores.shape, 1)
        scores = jnp.where(key_pos <= query_pos, scores, negative)
        expo = jnp.exp(scores - jnp.max(scores, axis=1, keepdims=True))
        total = jnp.sum(expo, axis=1, keepdims=True)
        mixed = jnp.dot(
            expo.astype(jnp.bfloat16), value_rows, preferred_element_type=jnp.float32
        )
        return mixed / total

    def attend(head):
        diff = one_map(queries_a, head, 0) - lambdas[head] * one_map(queries_b, head, span)
        norm = lax.rsqrt(jnp.mean(diff * diff, axis=1, keepdims=True) + eps)
        heads[:, head * VDIM : (head + 1) * VDIM] = (diff * norm * head_gain[...]).astype(
            jnp.bfloat16
        )

    def forward(k):
        core_copy(k).start()
        across_copy(k).start()

    def relay(k):
        across_copy(k).wait_recv()
        core_across_copy(k).start()

    def send_sums(k):
        pair_copy(k).wait_recv()
        sums[k] = (
            parts[k, 2].astype(jnp.float32) + pair_in[k].astype(jnp.float32)
        ).astype(jnp.bfloat16)
        sums_copy(k).start()

    def finish(k):
        part_and_sums(k).wait_recv()
        return (
            parts[k, 0].astype(jnp.float32)
            + part_in[0, k].astype(jnp.float32)
            + part_in[1, k].astype(jnp.float32)
        ).astype(jnp.bfloat16)

    def send_back(k):
        final[k] = finish(k)
        back_copy(k).start()

    def feed(k):
        both_core_copies(k).wait_recv()
        inputs = rows[k].reshape(flat, width)
        step = min(256, units)
        for first in range(0, units, step):
            gate = jnp.dot(
                inputs, gate_v[:, first : first + step], preferred_element_type=jnp.float32
            )
            up = jnp.dot(
                inputs, up_v[:, first : first + step], preferred_element_type=jnp.float32
            )
            hidden[:, first : first + step] = clamped_unit(gate, up).astype(jnp.bfloat16)
        for first in range(0, width, 256):
            piece = jnp.dot(
                hidden[...], down_v[:, first : first + 256], preferred_element_type=jnp.float32
            )
            parts[k, :, :, first : first + 256] = piece.astype(jnp.bfloat16).reshape(
                4, cap, 256
            )
        pair_copy(k).start()
        part_copy(k).start()

    barrier = pltpu.get_barrier_semaphore()
    for shift in range(1, n):
        pl.semaphore_signal(
            barrier, inc=1, device_id={"ep": (me + shift) % n}, device_id_type=MESH
        )
    for shift in range(1, 4):
        pl.semaphore_signal(
            barrier, inc=1, device_id={"tp": (tp + shift) % 4}, device_id_type=MESH
        )

    pairs = [
        (moe_tokens, tokens_in), (gain_in, moe_gain), (routes_in, routes),
        (keys_a, kv_all.at[me, :, 0:span]), (keys_b, kv_all.at[me, :, span : 2 * span]),
        (values, kv_all.at[me, :, 2 * span :]), (weights_in, route_weights),
        (w_gate, gate_v), (w_up, up_v), (w_down, down_v), (w_out, out_v),
        (queries_a_in, queries_a), (queries_b_in, queries_b), (head_gain_in, head_gain),
        (lambdas_in, lambdas),
    ]
    loads = [
        pltpu.make_async_copy(source, target, local.at[i])
        for i, (source, target) in enumerate(pairs)
    ]
    for load in loads:
        load.start()
    for load in loads[:3]:
        load.wait()

    inputs = tokens_in[...].astype(jnp.float32)
    normed = (
        inputs
        * lax.rsqrt(jnp.mean(inputs * inputs, axis=1, keepdims=True) + eps)
        * moe_gain[...]
    ).astype(jnp.bfloat16)
    count = tokens_in.shape[0]
    expert = lax.broadcasted_iota(jnp.int32, (n, count), 0)
    named = [routes[k : k + 1, :] == expert for k in range(TOP)]
    member = named[0]
    for k in range(1, TOP):
        member = member | named[k]
    earlier = lax.broadcasted_iota(jnp.int32, (count, count), 0) < lax.broadcasted_iota(
        jnp.int32, (count, count), 1
    )
    place = jnp.dot(
        jnp.where(member, 1.0, 0.0).astype(jnp.bfloat16),
        jnp.where(earlier, 1.0, 0.0).astype(jnp.bfloat16),
        preferred_element_type=jnp.float32,
    )
    position = lax.broadcasted_iota(jnp.int32, (cap, count), 0).astype(jnp.float32)
    slot = jnp.where(member, place, -1.0)
    for e in range(n):
        pick = jnp.where(slot[e : e + 1, :] == position, 1.0, 0.0).astype(jnp.bfloat16)
        outgoing[e] = jnp.dot(pick, normed, preferred_element_type=jnp.float32).astype(
            jnp.bfloat16
        )
    rows[0, 0] = outgoing[me]
    pl.semaphore_wait(barrier, n + 2)

    forward(0)
    for k in (1, 4):
        out_copy(k).start()
    out_copy(5 - 3 * inner).start()

    for other in range(1, floors):

        @pl.when(floor < other)
        def _():
            for side in range(2):
                kv_all[2 * other + side] = jnp.zeros(kv_all.shape[1:], jnp.bfloat16)

    for load in loads[3:7]:
        load.wait()
    share = route_weights[...]
    scale = jnp.where(named[0], share[0:1, :], 0.0)
    for k in range(1, TOP):
        scale = scale + jnp.where(named[k], share[k : k + 1, :], 0.0)
    table = jnp.concatenate(
        [
            jnp.where(slot[e : e + 1, :] == position, scale[e : e + 1, :], 0.0)
            for e in range(n)
        ],
        axis=0,
    ).T
    high = table.astype(jnp.bfloat16)
    weigh[0:count] = high
    weigh[count:] = (table - high.astype(jnp.float32)).astype(jnp.bfloat16)
    out_copy(2 + 3 * inner).start()
    for load in loads[7:]:
        load.wait()

    def kv_next(stage):
        @pl.when(floor >= stage)
        def _():
            kv_z_copy(stage).wait_recv()
            kv_y_copy(stage).start()
            if stage < floors - 1:

                @pl.when(floor < floors - 1)
                def _():
                    kv_z_copy(stage + 1).start()

    def pass_on(k):
        out_copy(k).wait_recv()
        forward(k)

    @pl.loop(0, n)
    def _(step):
        @pl.when(step == 3)
        def _():
            send_sums(1)

        @pl.when(step < 5)
        def _():
            pass_on(order(step + 1))

        for k in (6, 7):

            @pl.when(step == k - 2 + inner)
            def _():
                pass_on(k)

        for k in (4, 5):

            @pl.when(step == k + 1)
            def _():
                send_sums(k)

        @pl.when(step == 0)
        def _():
            out_copy(3).start()
            out_copy(6).start()

        @pl.when(step == 1)
        def _():
            out_copy(7).start()

        @pl.when(step == 3)
        def _():
            @pl.when(floor < floors - 1)
            def _():
                kv_z_copy(1).start()

            kv_y_copy(0).start()

        @pl.when(step == 5)
        def _():
            send_back(1)

        @pl.when(step == 6)
        def _():
            kv_next(1)

        @pl.when((step == 7) & (inner == 1))
        def _():
            send_sums(6)
            send_back(4)

        @pl.when(step == 7)
        def _():
            kv_next(2)

        relay(order(step))
        feed(order(step))

    @pl.when(inner == 0)
    def _():
        send_sums(6)

    send_sums(7)

    @pl.when(inner == 0)
    def _():
        send_back(4)

    send_back(5)
    send_sums(3)
    send_sums(2)
    kv_next(3)
    for stage in range(floors):

        @pl.when(floor >= stage)
        def _():
            kv_y_copy(stage).wait_recv()

    send_back(6)
    for head in range(local_heads):
        attend(head)
    for first in range(0, width, 256):
        piece = jnp.dot(
            heads[...], out_v[:, first : first + 256], preferred_element_type=jnp.float32
        )
        shares[:, :, first : first + 256] = piece.astype(jnp.bfloat16).reshape(
            4, tokens // 4, 256
        )
    mix_pair_copy.start()
    mix_part_copy.start()
    send_back(7)
    mix_pair_copy.wait_recv()
    mix_sum[...] = (
        shares[across].astype(jnp.float32) + mix_pair[...].astype(jnp.float32)
    ).astype(jnp.bfloat16)
    mix_sum_copy.start()
    send_sums(0)
    send_back(3)
    send_back(2)
    ret[me] = finish(0)

    all_back().wait_recv()
    for first in range(0, width, 256):
        table = ret[:, :, first : first + 256].reshape(n * cap, 256)
        total = jnp.dot(weigh[...], table, preferred_element_type=jnp.float32)
        moe_out[:, first : first + 256] = (total[:count] + total[count:]).astype(jnp.bfloat16)

    mix_part_copy.wait_recv()
    mix_sum_copy.wait_recv()
    mixer_out[...] = (
        shares[tp].astype(jnp.float32)
        + mix_part[...].astype(jnp.float32)
        + mix_in[...].astype(jnp.float32)
    ).astype(jnp.bfloat16)

    for made in (mix_part_copy, mix_pair_copy, mix_sum_copy):
        made.wait_send()
    for stage in range(1, floors):

        @pl.when((floor >= stage - 1) & (floor < floors - 1))
        def _():
            kv_z_copy(stage).wait_send()

    for stage in range(floors):

        @pl.when(floor >= stage)
        def _():
            kv_y_copy(stage).wait_send()

    for made in all_sent():
        made.wait_send()


def settle(first, second, first_out, second_out, sems):
    copies = [
        pltpu.make_async_copy(first, first_out, sems.at[0]),
        pltpu.make_async_copy(second, second_out, sems.at[1]),
    ]
    for made in copies:
        made.start()
    for made in copies:
        made.wait()


def run_exchange(
    n, cap, tokens_in, moe_gain, routes, route_weights, queries_a, queries_b, head_gain,
    lambdas, keys_a, keys_b, values, w_gate, w_up, w_down, w_out,
):
    count, width = tokens_in.shape
    units = w_gate.shape[1]
    block = (n, cap, width)
    tokens = keys_a.shape[0]
    kv_width = keys_a.shape[1] + keys_b.shape[1] + values.shape[1]
    quarter = (tokens // 4, width)
    vmem = pl.BlockSpec(memory_space=pltpu.VMEM)
    hbm = pl.BlockSpec(memory_space=pltpu.HBM)
    call = pl.pallas_call(
        functools.partial(exchange, n),
        out_shape=(
            pltpu.VMEM((count, width), jnp.bfloat16),
            pltpu.VMEM(quarter, jnp.bfloat16),
        ),
        in_specs=[hbm] * 15,
        out_specs=(vmem, vmem),
        scratch_shapes=[
            pltpu.VMEM(tokens_in.shape, jnp.bfloat16),
            pltpu.VMEM((1, width), jnp.float32),
            pltpu.VMEM((TOP, count), jnp.int32),
            pltpu.VMEM((TOP, count), jnp.float32),
            pltpu.VMEM(queries_a.shape, jnp.bfloat16),
            pltpu.VMEM(queries_b.shape, jnp.bfloat16),
            pltpu.VMEM((1, VDIM), jnp.float32),
            pltpu.SMEM(lambdas.shape, jnp.float32),
            pltpu.VMEM(block, jnp.bfloat16),
            pltpu.VMEM(block, jnp.bfloat16),
            pltpu.VMEM((2 * count, n * cap), jnp.bfloat16),
            pltpu.VMEM((n, 4, cap, width), jnp.bfloat16),
            pltpu.VMEM((n, 4, cap, width), jnp.bfloat16),
            pltpu.VMEM((2,) + block, jnp.bfloat16),
            pltpu.VMEM(block, jnp.bfloat16),
            pltpu.VMEM(block, jnp.bfloat16),
            pltpu.VMEM(block, jnp.bfloat16),
            pltpu.VMEM((4 * cap, units), jnp.bfloat16),
            pltpu.VMEM(w_gate.shape, jnp.bfloat16),
            pltpu.VMEM(w_up.shape, jnp.bfloat16),
            pltpu.VMEM(w_down.shape, jnp.bfloat16),
            pltpu.VMEM(w_out.shape, jnp.bfloat16),
            pltpu.VMEM((n, tokens, kv_width), jnp.bfloat16),
            pltpu.VMEM((tokens, w_out.shape[0]), jnp.bfloat16),
            pltpu.VMEM((4,) + quarter, jnp.bfloat16),
            pltpu.VMEM(quarter, jnp.bfloat16),
            pltpu.VMEM(quarter, jnp.bfloat16),
            pltpu.VMEM(quarter, jnp.bfloat16),
            pltpu.VMEM(quarter, jnp.bfloat16),
            pltpu.SemaphoreType.DMA((15,)),
            pltpu.SemaphoreType.DMA((5 * n + 13,)),
            pltpu.SemaphoreType.DMA((15,)),
        ],
        compiler_params=pltpu.CompilerParams(
            collective_id=0, has_side_effects=True, vmem_limit_bytes=48 * 2**20
        ),
        name="exchange",
    )
    operands = (
        tokens_in, moe_gain.reshape(1, -1), routes.T, route_weights.T,
        queries_a, queries_b, head_gain.reshape(1, -1), lambdas,
        keys_a, keys_b, values, w_gate, w_up, w_down, w_out,
    )
    made = call(*[pltpu.with_memory_space_constraint(x, pltpu.HBM) for x in operands])
    return pl.pallas_call(
        settle,
        out_shape=tuple(jax.ShapeDtypeStruct(x.shape, x.dtype) for x in made),
        in_specs=[vmem] * 2,
        out_specs=(hbm, hbm),
        scratch_shapes=[pltpu.SemaphoreType.DMA((2,))],
        compiler_params=pltpu.CompilerParams(vmem_limit_bytes=2**20),
        name="settle",
    )(*[pltpu.with_memory_space_constraint(x, pltpu.VMEM) for x in made])


def fast_body(
    queries_a, queries_b, keys_a, keys_b, values, lambdas, head_gain, w_out,
    moe_tokens, moe_gain, routes, route_weights, w_gate, w_up, w_down,
):
    n = lax.axis_size("ep")
    cap = 3 * moe_tokens.shape[0] * TOP // (2 * n)
    moe_out, mixer_out = run_exchange(
        n, cap, moe_tokens, moe_gain, routes, route_weights, queries_a, queries_b,
        head_gain, lambdas, keys_a, keys_b, values, w_gate[0], w_up[0], w_down[0], w_out,
    )
    return (mixer_out, moe_out)


def whole_body(*args):
    n, n_tp = lax.axis_size("ep"), lax.axis_size("tp")
    tok_rows, w_gate = args[8].shape[0], args[12]
    cap = 3 * tok_rows * TOP // (2 * n)
    if w_gate.shape[0] == 1 and n_tp == 4 and n == 8 and cap % 16 == 0:
        return fast_body(*args)
    return body(*args)


def solution(mesh):
    return jax.shard_map(
        whole_body,
        mesh=mesh,
        in_specs=(
            P("ep", "tp"),
            P("ep", "tp"),
            P("ep", "tp"),
            P("ep", "tp"),
            P("ep", "tp"),
            P("tp"),
            P(),
            P("tp", None),
            P(("ep", "tp"), None),
            P(),
            P(("ep", "tp"), None),
            P(("ep", "tp"), None),
            P("ep", None, "tp"),
            P("ep", None, "tp"),
            P("ep", "tp", None),
        ),
        out_specs=(P(("ep", "tp"), None), P(("ep", "tp"), None)),
        check_vma=False,
    )
```
